512 devices in a mesh: sp: 32 (over z, core), tp: 16 (over y, x).
Axes of the slice: x: 4, y: 4, z: 16, core: 2. Of those that a mesh axis runs over, the one named last changes fastest.
Arguments:
- residual_in: bfloat16 [8192, 2048], P('sp'), may hold values from -6 to 6
- queries: bfloat16 [8192, 2048], P('sp', 'tp'), may hold values from -6 to 4
- keys: bfloat16 [8192, 2048], P('sp', 'tp'), may hold values from -4 to 5.2
- values: bfloat16 [8192, 2048], P('sp', 'tp'), may hold values from -9.5 to 9.5
- out_weight: bfloat16 [2048, 2048], P('tp'), may hold values from -0.125 to 0.125
- norm_gain: float32 [2048], replicated, may hold values from 0.1 to 1.9
- expert_routes: int32 [8192, 2], P('sp'), may hold values from 0 to 31, all different within a row; in each aligned block of 256 rows (0 to 255, 256 to 511, ...) at most 32 rows name the same one
- route_scores: float32 [8192, 2], P('sp'), may hold values from -6 to 6
- gate_weight: bfloat16 [32, 2048, 4096], P('sp', None, 'tp'), may hold values from -0.125 to 0.125
- up_weight: bfloat16 [32, 2048, 4096], P('sp', None, 'tp'), may hold values from -0.125 to 0.125
- down_weight: bfloat16 [32, 4096, 2048], P('sp', 'tp'), may hold values from -0.09375 to 0.09375
Outputs:
- layer_out: bfloat16 [8192, 2048], P('sp', 'tp')
The draws below stay inside these ranges and needn't reach their ends.
Inputs may be any that keep to these rules, and one draw needn't show every extreme that they name: `expert_routes`: each row names 2 different experts; among the 256 rows of one index of sp no expert is named more than 32 times, and in every draw some such block names some expert exactly 32 times.
All inputs are finite; a program needn't handle non-finite values.
Results may differ from the reference program's by a relative error of at most 0.015.
Values may be sent and summed in bfloat16 or wider, within the bound.
No kernel may reach another device: no remote copies, remote signals or barrier semaphores. Data moves between devices by JAX's collectives and lax.ppermute only.
A program may use at most 64 MiB of HBM per device.

```python
import math
from functools import partial
import jax
import jax.numpy as jnp
import numpy as np
from jax import lax

D = 2048
HEADS = 32
HD = 64
FF = 4096
TOP = 2
TOKENS_PER_SHARD = 256
SEQUENCE_LENGTH = 8192
EXPERTS = 32
CAP = 32
N_SP = 32
N_TP = 16


def draw_queries(key, part):
    key_fast, jitter_key = jax.random.split(jax.random.fold_in(key, 11))
    slow_mean = -(jnp.log(jnp.float32(SEQUENCE_LENGTH)) + 2.0) / math.sqrt(HD)
    fast_mean = -5.5 / math.sqrt(HD)
    fast = jax.random.bernoulli(key_fast, 0.5, (HEADS,))
    noise = jnp.clip(jax.random.normal(jitter_key, (SEQUENCE_LENGTH, HEADS, HD), jnp.float32), -4.0, 4.0)
    center_values = jnp.where(fast, fast_mean, slow_mean)
    return (center_values[None, :, None] + noise).reshape(SEQUENCE_LENGTH, HEADS * HD).astype(jnp.bfloat16)


def draw_keys(key, part):
    baseline_key, spike_key, jitter_key = jax.random.split(jax.random.fold_in(key, 23), 3)
    baseline_level = jax.random.uniform(baseline_key, (SEQUENCE_LENGTH // TOKENS_PER_SHARD,), jnp.float32, 0.9, 1.1)
    spike_positions = jax.random.randint(spike_key, (8,), 0, SEQUENCE_LENGTH)
    spike_pattern = jnp.zeros((SEQUENCE_LENGTH,), jnp.float32).at[spike_positions].set(1.0)
    center_values = jnp.repeat(baseline_level, TOKENS_PER_SHARD) * (1.0 - spike_pattern)
    noise = jnp.clip(jax.random.normal(jitter_key, (SEQUENCE_LENGTH, HEADS * HD), jnp.float32), -4.0, 4.0)
    return (center_values[:, None] + noise).astype(jnp.bfloat16)


def draw_values(key, part):
    key_offset = jax.random.fold_in(jax.random.fold_in(key, 37), 0)
    jitter_key = jax.random.fold_in(jax.random.fold_in(key, 37), 2)
    offset = jnp.clip(2.0 * jax.random.normal(key_offset, (SEQUENCE_LENGTH // TOKENS_PER_SHARD, HEADS * HD), jnp.float32), -5.0, 5.0)
    noise = jnp.clip(jax.random.normal(jitter_key, (SEQUENCE_LENGTH, HEADS * HD), jnp.float32), -4.0, 4.0)
    return (jnp.repeat(offset, TOKENS_PER_SHARD, axis=0) + noise).astype(jnp.bfloat16)


def block_scale(key, shape, shards, low, top_value):
    def one(dim, shards_of):
        heights = jax.random.uniform(jax.random.fold_in(jax.random.fold_in(key, 6), dim), (shards_of,), jnp.float32, low / len(shards), top_value / len(shards))
        return jnp.repeat(jnp.exp(heights), shape[dim] // shards_of).reshape((-1,) + (1,) * (len(shape) - dim - 1))

    factor_of = one(*shards[0])
    for cut in shards[1:]:
        factor_of = factor_of * one(*cut)
    return factor_of


def deal_out(rng, own, number, rows, count, top, most, skew):
    ranking = jax.random.permutation(rng, count)
    packed, usual = load_shares(count, rows * top, most, skew, True), load_shares(count, rows * top, most, skew, False)
    places = jnp.arange(count)

    def named(sizes, rotation):
        used = int((sizes > 0).sum())
        fixed = max(1, used // 4)
        passed = fixed + (places - fixed + rotation * (used - fixed)) % max(1, count - fixed)
        return jnp.zeros((count,), jnp.int32).at[ranking[jnp.where(places < fixed, places, passed)]].set(jnp.asarray(sizes, jnp.int32))

    sizes = jnp.where(number % 4 == 0, named(packed, number // 4), named(usual, number - number // 4 - 1))
    mixed = jax.random.permutation(jax.random.fold_in(own, 3), count)
    giver, sink = mixed[0:count // 2 * 2:2], mixed[1:count // 2 * 2:2]
    room = jnp.minimum(sizes[giver] - 1, most - sizes[sink]) // 2
    room = jnp.where((giver == ranking[0]) | (sink == ranking[0]) | (sizes[sink] == 0), 0, jnp.maximum(room, 0))
    passed = jax.random.randint(jax.random.fold_in(own, 4), (count // 2,), 0, 1 << 20) % (room + 1)
    sizes = sizes.at[giver].add(-passed).at[sink].add(passed)
    items = jnp.searchsorted(jnp.cumsum(sizes), jnp.arange(rows * top), side="right").astype(jnp.int32)
    listing = items.reshape(top, rows).T
    listing = listing[jax.random.permutation(jax.random.fold_in(own, 1), rows)]
    rotation = jax.random.randint(jax.random.fold_in(own, 2), (rows, 1), 0, top)
    return jnp.take_along_axis(listing, (jnp.arange(top)[None, :] + rotation) % top, axis=1)


def load_shares(count, total, bound, skew, full):
    loads = [(1 << 20) // math.isqrt(rank ** skew) + 1 for rank in range(1, count + 1)]
    largest = bound if full else min(bound, max(-(-total // count), total * loads[0] // sum(loads)))
    least = 1 if total - largest >= count - 1 else 0
    given, spare = [largest] + [least] * (count - 1), total - largest - least * (count - 1)
    while spare > 0:
        free = [i for i in range(1, count) if given[i] < largest] or [i for i in range(1, count) if given[i] < bound]
        mass, budget = sum([loads[i] for i in free]), spare
        for i in free:
            addition = min(bound - given[i], max(1, budget * loads[i] // mass), spare)
            given[i] = given[i] + addition
            spare = spare - addition
    return np.array(given)


def normal_values(stream_key, shape, spread, limit, cuts=(), held_as=jnp.bfloat16):
    entries = jax.random.normal(stream_key, shape, jnp.float32) * spread
    if len(cuts) > 0:
        entries = block_scale(stream_key, shape, cuts, -0.22, 0.18) * entries
    return jnp.clip(entries, min=-limit, max=limit).astype(held_as)


def setup_inputs(seed: int = 0) -> dict:
    streams_of = jax.random.split(jax.random.key(seed), 12)
    residual_in = normal_values(streams_of[0], (SEQUENCE_LENGTH, D), 1.0, 6.0, ((0, 32),))
    queries = draw_queries(jax.random.fold_in(streams_of[11], 71), 0)
    keys = draw_keys(jax.random.fold_in(streams_of[11], 71), 0)
    values = draw_values(jax.random.fold_in(streams_of[11], 71), 0)
    out_weight = normal_values(streams_of[4], (HEADS * HD, D), (HEADS * HD) ** -0.5, 0.125, ((0, 16),))
    norm_gain = jnp.clip(1.0 + 0.18 * jax.random.normal(streams_of[5], (D,), jnp.float32), 0.1, 1.9)
    expert_routes_keys = jax.random.split(jax.random.fold_in(streams_of[6], 1), SEQUENCE_LENGTH // TOKENS_PER_SHARD)
    expert_routes_turns = jax.random.permutation(jax.random.fold_in(streams_of[6], 3), SEQUENCE_LENGTH // TOKENS_PER_SHARD)
    expert_routes = jax.vmap(lambda own, number: deal_out(jax.random.fold_in(streams_of[6], 2), own, number, TOKENS_PER_SHARD, EXPERTS, TOP, CAP, 2))(expert_routes_keys, expert_routes_turns).reshape((SEQUENCE_LENGTH, TOP))
    route_scores = normal_values(streams_of[7], (SEQUENCE_LENGTH, TOP), 1.5, 6.0, ((0, 32),), jnp.float32)
    gate_weight = normal_values(streams_of[8], (EXPERTS, D, FF), D ** -0.5, 0.125, ((0, 32), (2, 16)))
    up_weight = normal_values(streams_of[9], (EXPERTS, D, FF), D ** -0.5, 0.125, ((0, 32), (2, 16)))
    down_weight = normal_values(streams_of[10], (EXPERTS, FF, D), FF ** -0.5, 0.09375, ((0, 32), (1, 16)))
    return dict(residual_in=residual_in, queries=queries, keys=keys, values=values, out_weight=out_weight, norm_gain=norm_gain, expert_routes=expert_routes, route_scores=route_scores, gate_weight=gate_weight, up_weight=up_weight, down_weight=down_weight)


epsilon = 1e-06

def rounded_groups(left, right, groups):
    width = left.shape[1] // groups

    def add_group(total, group_index):
        part_left = lax.dynamic_slice_in_dim(left, group_index * width, width, 1)
        part_right = lax.dynamic_slice_in_dim(right, group_index * width, width, 0)
        term = jnp.dot(part_left, part_right, preferred_element_type=jnp.float32).astype(jnp.bfloat16)
        term = lax.optimization_barrier(term)
        return (total + term.astype(jnp.float32), None)
    start_total = jnp.zeros((left.shape[0], right.shape[1]), jnp.float32)
    total, unused = lax.scan(add_group, start_total, jnp.arange(groups, dtype=jnp.int32))
    return total

def stick_attention(queries, keys, values):
    total_len = queries.shape[0]
    span = min(512, total_len)
    scale = HD ** (-0.5)
    q_heads = queries.reshape(total_len, HEADS, HD).transpose(1, 0, 2)
    k_heads = keys.reshape(total_len, HEADS, HD).transpose(1, 0, 2)
    v_heads = values.reshape(total_len, HEADS, HD).transpose(1, 0, 2)
    pieces = []
    for block_start in range(0, total_len, span):
        block_stop = block_start + span
        query_pos = block_start + jnp.arange(span, dtype=jnp.int32)
        key_pos = jnp.arange(block_stop, dtype=jnp.int32)
        causal = key_pos[None, :] < query_pos[:, None]

        def one_head(operands):
            q_part, k_part, v_part = operands
            scores = jnp.dot(q_part, k_part.T, preferred_element_type=jnp.float32) * scale
            log_keep = jnp.where(causal, jax.nn.log_sigmoid(-scores), 0.0)
            between = lax.cumsum(log_keep, axis=1, reverse=True) - log_keep
            weights = jnp.where(causal, jnp.exp(jax.nn.log_sigmoid(scores) + between), 0.0).astype(jnp.bfloat16)
            return jnp.dot(weights, v_part, preferred_element_type=jnp.float32)
        pieces.append(lax.map(one_head, (q_heads[:, block_start:block_stop], k_heads[:, :block_stop], v_heads[:, :block_stop])))
    joined = jnp.concatenate(pieces, axis=1)
    return joined.transpose(1, 0, 2).reshape(total_len, HEADS * HD).astype(jnp.bfloat16)

def route_targets(routes, experts, capacity):
    flat_routes = routes.reshape(-1)
    onehot = (flat_routes[:, None] == jnp.arange(experts, dtype=jnp.int32)[None, :]).astype(jnp.int32)
    before = jnp.cumsum(onehot, axis=0) - onehot
    return flat_routes * capacity + lax.optimization_barrier(jnp.sum(before * onehot, axis=1))

def run_expert(operands):
    rows_in, gate_part, up_part, down_part = operands
    gate_act = jnp.dot(rows_in, gate_part, preferred_element_type=jnp.float32)
    up_act = jnp.dot(rows_in, up_part, preferred_element_type=jnp.float32)
    hidden = (jax.nn.silu(gate_act) * up_act).astype(jnp.bfloat16)
    return rounded_groups(hidden, down_part, N_TP).astype(jnp.bfloat16)

def reference(residual_in, queries, keys, values, out_weight, norm_gain, expert_routes, route_scores, gate_weight, up_weight, down_weight):
    mixed_heads = stick_attention(queries, keys, values)
    attended = rounded_groups(mixed_heads, out_weight, N_TP).astype(jnp.bfloat16)
    stream = (residual_in.astype(jnp.float32) + attended.astype(jnp.float32)).astype(jnp.bfloat16)
    stream_wide = stream.astype(jnp.float32)
    normed = (stream_wide * lax.rsqrt(lax.optimization_barrier(jnp.mean(stream_wide * stream_wide, axis=1, keepdims=True)) + epsilon) * norm_gain).astype(jnp.bfloat16)
    block_targets = jax.vmap(partial(route_targets, experts=EXPERTS, capacity=CAP))(expert_routes.reshape(N_SP, TOKENS_PER_SHARD, TOP))
    block_ids = jnp.arange(N_SP, dtype=jnp.int32)[:, None]
    global_slots = block_targets // CAP * (N_SP * CAP) + block_ids * CAP + block_targets % CAP
    owners = block_ids * TOKENS_PER_SHARD + jnp.arange(TOKENS_PER_SHARD * TOP, dtype=jnp.int32)[None, :] // TOP
    slot_owner = jnp.full((EXPERTS * N_SP * CAP,), SEQUENCE_LENGTH, jnp.int32).at[global_slots.reshape(-1)].set(owners.reshape(-1))
    padded = jnp.concatenate([normed, jnp.zeros((1, D), jnp.bfloat16)], axis=0)
    gathered = padded[slot_owner].reshape(EXPERTS, N_SP * CAP, D)
    outputs = lax.map(run_expert, (gathered, gate_weight, up_weight, down_weight))
    results = outputs.reshape(EXPERTS * N_SP * CAP, D)
    picked = results[global_slots.reshape(-1)].astype(jnp.float32).reshape(SEQUENCE_LENGTH, TOP, D)
    shares = jax.nn.sigmoid(route_scores - route_scores[:, ::-1])
    combined = lax.optimization_barrier(jnp.sum(picked * shares[:, :, None], axis=1))
    return (stream_wide + combined).astype(jnp.bfloat16)
```

```python
import functools

import jax
import jax.numpy as jnp
from jax import lax
from jax.experimental import pallas as pl
from jax.experimental.pallas import tpu as pltpu
from jax.sharding import Mesh, PartitionSpec as P

HD = 64
LANES = 128
ROWS = 256
EPSILON = 1e-06
BF = jnp.bfloat16
F32 = jnp.float32
VM = pl.BlockSpec(memory_space=pltpu.VMEM)
SM = pl.BlockSpec(memory_space=pltpu.SMEM)


def call(body, out_shape, specs, **more):
    return pl.pallas_call(body, out_shape=out_shape, in_specs=specs, **more)


def shaped(dims, dtype=BF):
    return jax.ShapeDtypeStruct(dims, dtype)


def lane_ids(dims):
    return lax.broadcasted_iota(jnp.int32, dims, len(dims) - 1)


def dot(a, b):
    return jnp.dot(a, b, preferred_element_type=F32)


def pack_body(q_ref, k_ref, v_ref, out_ref):
    q, k, v = (r[...].astype(F32) for r in (q_ref, k_ref, v_ref))
    low = lane_ids(q.shape) < HD
    q = q * (HD**-0.5)
    q_turned, k_turned, v_turned = (pltpu.roll(a, HD, 1) for a in (q, k, v))
    out_ref[0, 0] = jnp.where(low, k, v_turned).astype(BF)
    out_ref[1, 0] = jnp.where(low, k_turned, v).astype(BF)
    out_ref[0, 1] = jnp.where(low, q, 0.0).astype(BF)
    out_ref[1, 1] = jnp.where(low, q_turned, 0.0).astype(BF)


def tile(q, kv, later, mask):
    z = lax.dot_general(q, kv, (((1,), (1,)), ((), ())), preferred_element_type=F32)
    if mask is not None:
        z = jnp.where(mask, z, -1e30)
    kept = jnp.maximum(z, jnp.log(1.0 + jnp.exp(jnp.minimum(z, 80.0))))
    after = dot(kept.astype(BF), later)
    weights = jnp.exp((z - kept) - after).astype(BF)
    return dot(weights, kv), after[:, :1] + kept[:, :1]


def attend_body(z_ref, q_ref, kv_ref, later_ref, out_ref, *, step):
    z = z_ref[0]
    later = later_ref[...]
    causal = lane_ids((ROWS, ROWS)) < lax.broadcasted_iota(jnp.int32, (ROWS, ROWS), 0)
    parts = 2 * ROWS // step
    qs = [q_ref[i * step : (i + 1) * step] for i in range(parts)]
    base = z * (2 * ROWS)
    kv0 = kv_ref[pl.ds(pl.multiple_of(base, ROWS), ROWS)]
    kv1 = kv_ref[pl.ds(pl.multiple_of(base + ROWS, ROWS), ROWS)]
    state = []
    for i in range(parts):
        half, at = divmod(i * step, ROWS)
        mask = causal[at : at + step]
        if half == 0:
            out, total = tile(qs[i], kv0, later, mask)
        else:
            out, total = tile(qs[i], kv1, later, mask)
            more, further = tile(qs[i], kv0, later, None)
            out, total = out + jnp.exp(-total) * more, total + further
        state.append((out, total))

    def one(j, state):
        at = pl.multiple_of((2 * z - 1 - j) * ROWS, ROWS)
        kv = kv_ref[pl.ds(at, ROWS)]
        new = []
        for q, (out, total) in zip(qs, state):
            more, further = tile(q, kv, later, None)
            new.append((out + jnp.exp(-total) * more, total + further))
        return tuple(new)

    state = lax.fori_loop(0, 2 * z, one, tuple(state))
    outs = jnp.concatenate([s[0] for s in state], axis=0)
    low = lane_ids((ROWS // 2, LANES)) < HD
    for block in range(2):
        top = outs[block * ROWS : block * ROWS + ROWS // 2]
        bottom = outs[block * ROWS + ROWS // 2 : (block + 1) * ROWS]
        both = jnp.where(low, pltpu.roll(top, HD, 1), bottom).astype(BF)
        for peer in range(out_ref.shape[1]):
            out_ref[block, peer] = both


def route_body(col_ref, row_ref, col_out, row_out, *, experts, cap):
    below = (lane_ids((ROWS, ROWS)) < lax.broadcasted_iota(jnp.int32, (ROWS, ROWS), 0)).astype(F32).astype(BF)
    above = (lane_ids((ROWS, ROWS)) > lax.broadcasted_iota(jnp.int32, (ROWS, ROWS), 0)).astype(F32).astype(BF)
    ids = lane_ids((ROWS, LANES))
    hot = [(ids == col_ref[:, k : k + 1]).astype(F32) for k in range(2)]
    before = dot(below, (hot[0] + hot[1]).astype(BF))
    for k in range(2):
        place = jnp.sum(before * hot[k], axis=1, keepdims=True).astype(jnp.int32)
        col_out[:, k : k + 1] = col_ref[:, k : k + 1] * cap + place
    ids = lax.broadcasted_iota(jnp.int32, (experts, ROWS), 0)
    hot = [(ids == row_ref[k : k + 1]).astype(F32) for k in range(2)]
    before = dot((hot[0] + hot[1]).astype(BF), above)
    for k in range(2):
        place = jnp.sum(before * hot[k], axis=0, keepdims=True).astype(jnp.int32)
        row_out[k : k + 1] = row_ref[k : k + 1] * cap + place


def project_body(mixed_ref, ow_ref, res_ref, row_ref, stream_ref, out_ref):
    tp = ow_ref.shape[0]
    nothing = jnp.zeros((HD, LANES), BF)
    total = jnp.zeros((ROWS // 2, 2 * LANES), F32)
    for t in range(tp):
        pieces, weights = [], []
        for c in range(2):
            w = ow_ref[t, c * HD : (c + 1) * HD]
            pieces.append(mixed_ref[c * tp + t])
            weights.append(jnp.concatenate([w, nothing], axis=1))
            weights.append(jnp.concatenate([nothing, w], axis=1))
        total = total + dot(jnp.concatenate(pieces, axis=1), jnp.concatenate(weights, axis=0))
    attended = jnp.concatenate([total[:, :LANES], total[:, LANES:]], axis=0).astype(BF)
    stream = (res_ref[...].astype(F32) + attended.astype(F32)).astype(BF)
    stream_ref[...] = stream
    slots = lax.broadcasted_iota(jnp.int32, (out_ref.shape[0], ROWS), 0)
    owned = (slots == row_ref[0:1]) | (slots == row_ref[1:2])
    out_ref[...] = dot(owned.astype(F32).astype(BF), stream).astype(BF)


def expert_body(x_ref, gain_ref, gate_ref, up_ref, down_ref, out_ref):
    tp, rows = x_ref.shape[0], x_ref.shape[1]
    wide = [x_ref[i].astype(F32) for i in range(tp)]
    squares = wide[0] * wide[0]
    for w in wide[1:]:
        squares = squares + w * w
    mean = jnp.sum(squares, axis=1, keepdims=True) * (1.0 / (tp * LANES))
    factor = lax.rsqrt(mean + EPSILON)
    normed = [(w * factor * gain_ref[i : i + 1]).astype(BF) for i, w in enumerate(wide)]
    normed = jnp.concatenate(normed, axis=1)
    gate = dot(normed, gate_ref[...])
    up = dot(normed, up_ref[...])
    hidden = (gate / (1.0 + jnp.exp(-gate)) * up).astype(BF)
    for i in range(tp):
        out_ref[i] = dot(hidden, down_ref[:, i * LANES : (i + 1) * LANES]).astype(BF)


def sum_body(x_ref, out_ref):
    total = x_ref[0].astype(F32)
    for i in range(1, x_ref.shape[0]):
        total = total + x_ref[i].astype(F32)
    out_ref[...] = total.astype(BF)


def combine_body(x_ref, col_ref, score_ref, stream_ref, out_ref):
    x = x_ref[...]
    slots = lane_ids((ROWS, x.shape[0]))
    gap = score_ref[:, 0:1] - score_ref[:, 1:2]
    total = 0.0
    for k in range(2):
        owned = (slots == col_ref[:, k : k + 1]).astype(F32).astype(BF)
        share = 1.0 / (1.0 + jnp.exp(-gap if k == 0 else gap))
        total = total + share * dot(owned, x)
    out_ref[...] = (stream_ref[...].astype(F32) + total).astype(BF)


def shards(residual_in, queries, keys, values, out_weight, norm_gain, expert_routes, route_scores, gate_weight, up_weight, down_weight):
    zs, tp = lax.axis_size("z"), lax.axis_size("tp")
    experts = 2 * zs
    cap = 4 * ROWS // experts
    slots = experts * cap
    width = residual_in.shape[1]
    here = lax.axis_index("tp")

    packed = call(pack_body, shaped((2, 2, ROWS, LANES)), [VM] * 3)(queries, keys, values)
    packed = lax.all_to_all(packed, "core", 0, 0, tiled=True)
    own_kv = packed[:, 0].reshape(2 * ROWS, LANES)
    own_q = packed[:, 1].reshape(2 * ROWS, LANES)
    kv = lax.all_gather(own_kv, "z", axis=0, tiled=True)

    own_ow = jnp.moveaxis(out_weight.reshape(LANES, tp, LANES), 1, 0)
    own_ow = lax.all_to_all(own_ow, "tp", 0, 0, tiled=True)
    to_col, to_row = call(
        functools.partial(route_body, experts=experts, cap=cap),
        [shaped((ROWS, 2), jnp.int32), shaped((2, ROWS), jnp.int32)],
        [VM] * 2,
        out_specs=[VM] * 2,
    )(expert_routes, expert_routes.T)
    own_res = lax.dynamic_slice_in_dim(residual_in, here * LANES, LANES, 1)

    later = (lax.iota(jnp.int32, ROWS)[:, None] > lax.iota(jnp.int32, ROWS)[None, :]).astype(BF)
    place = lax.axis_index("z").reshape(1).astype(jnp.int32)
    mixed = call(
        functools.partial(attend_body, step=128),
        shaped((2, tp, ROWS // 2, LANES)),
        [SM, VM, VM, VM],
    )(place, own_q, kv, later)
    mixed = lax.all_to_all(mixed.reshape(2 * tp, ROWS // 2, LANES), ("core", "tp"), 0, 0, tiled=True)

    stream, outgoing = call(
        project_body,
        [shaped((ROWS, LANES)), shaped((slots, LANES))],
        [VM] * 4,
        out_specs=[VM] * 2,
    )(mixed, own_ow, own_res, to_row)
    arrived = lax.all_to_all(outgoing.reshape(experts, cap, LANES), ("z", "core"), 0, 0, tiled=True)
    copies = jnp.broadcast_to(arrived.reshape(1, slots, LANES), (tp, slots, LANES))
    arrived = lax.all_to_all(copies, "tp", 0, 0, tiled=True)

    chunk = 256
    whole = lambda i: (0, 0)
    parts = pl.pallas_call(
        expert_body,
        out_shape=shaped((tp, slots, LANES)),
        grid=(slots // chunk,),
        in_specs=[
            pl.BlockSpec((tp, chunk, LANES), lambda i: (0, i, 0)),
            pl.BlockSpec((tp, LANES), whole),
            pl.BlockSpec(gate_weight.shape[1:], whole),
            pl.BlockSpec(up_weight.shape[1:], whole),
            pl.BlockSpec(down_weight.shape[1:], whole),
        ],
        out_specs=pl.BlockSpec((tp, chunk, LANES), lambda i: (0, i, 0)),
    )(arrived, norm_gain.reshape(tp, LANES), gate_weight[0], up_weight[0], down_weight[0])
    parts = lax.all_to_all(parts, "tp", 0, 0, tiled=True)
    summed = pl.pallas_call(
        sum_body,
        out_shape=shaped((slots, LANES)),
        grid=(slots // chunk,),
        in_specs=[pl.BlockSpec((tp, chunk, LANES), lambda i: (0, i, 0))],
        out_specs=pl.BlockSpec((chunk, LANES), lambda i: (i, 0)),
    )(parts)
    returned = lax.all_to_all(summed.reshape(experts, cap, LANES), ("z", "core"), 0, 0, tiled=True)
    return call(combine_body, shaped((ROWS, LANES)), [VM] * 4)(
        returned.reshape(slots, LANES), to_col, route_scores, stream
    )


def solution(mesh):
    sp, tp = mesh.devices.shape
    fine = Mesh(mesh.devices.reshape(sp // 2, 2, tp), ("z", "core", "tp"))
    rows = ("z", "core")
    in_specs = (
        P(rows, None),
        P(rows, "tp"),
        P(rows, "tp"),
        P(rows, "tp"),
        P("tp", None),
        P(),
        P(rows, None),
        P(rows, None),
        P(rows, None, "tp"),
        P(rows, None, "tp"),
        P(rows, "tp", None),
    )
    return jax.shard_map(shards, mesh=fine, in_specs=in_specs, out_specs=P(rows, "tp"), check_vma=False)
```

```python
import functools

import jax
import jax.numpy as jnp
from jax import lax
from jax.experimental import pallas as pl
from jax.experimental.pallas import tpu as pltpu
from jax.sharding import Mesh, PartitionSpec as P

HD = 64
LANES = 128
ROWS = 256
EPSILON = 1e-06
BF = jnp.bfloat16
F32 = jnp.float32
VM = pl.BlockSpec(memory_space=pltpu.VMEM)
SM = pl.BlockSpec(memory_space=pltpu.SMEM)


def call(body, out_shape, specs, **more):
    return pl.pallas_call(body, out_shape=out_shape, in_specs=specs, **more)


def shaped(dims, dtype=BF):
    return jax.ShapeDtypeStruct(dims, dtype)


def lane_ids(dims):
    return lax.broadcasted_iota(jnp.int32, dims, len(dims) - 1)


def dot(a, b):
    return jnp.dot(a, b, preferred_element_type=F32)


def pack_body(q_ref, k_ref, v_ref, out_ref):
    q, k, v = (r[...].astype(F32) for r in (q_ref, k_ref, v_ref))
    low = lane_ids(q.shape) < HD
    q = q * (HD**-0.5)
    q_turned, k_turned, v_turned = (pltpu.roll(a, HD, 1) for a in (q, k, v))
    out_ref[0, 0] = jnp.where(low, k, v_turned).astype(BF)
    out_ref[1, 0] = jnp.where(low, k_turned, v).astype(BF)
    out_ref[0, 1] = jnp.where(low, q, 0.0).astype(BF)
    out_ref[1, 1] = jnp.where(low, q_turned, 0.0).astype(BF)


def scores(q, kv):
    return lax.dot_general(q, kv, (((1,), (1,)), ((), ())), preferred_element_type=F32)


def attend_body(z_ref, q_ref, kv_ref, later_ref, out_ref, *scratch):
    score_s, gap_s, kept_s, weight_s = (scratch[2 * i : 2 * i + 2] for i in range(4))
    acc_s, total_s = scratch[8:]
    z = z_ref[0]
    rows, chunk = 2 * ROWS, 64
    causal = lane_ids((ROWS, ROWS)) < lax.broadcasted_iota(jnp.int32, (ROWS, ROWS), 0)

    def keys_of(j):
        return kv_ref[pl.ds(pl.multiple_of(j * ROWS, ROWS), ROWS)]

    def tile(slot, kv, low, masks, first):
        for at in range(low, rows, chunk):
            s = score_s[slot][at : at + chunk]
            if at - low < len(masks) * chunk:
                s = jnp.where(masks[(at - low) // chunk], s, -1e30)
            kept = jnp.maximum(s, jnp.log(1.0 + jnp.exp(jnp.minimum(s, 80.0))))
            gap_s[slot][at : at + chunk] = s - kept
            kept_s[slot][at : at + chunk] = kept.astype(BF)
        after = dot(kept_s[slot][low:], later_ref[...])
        for at in range(low, rows, chunk):
            own = after[at - low : at - low + chunk]
            weight_s[slot][at : at + chunk] = jnp.exp(gap_s[slot][at : at + chunk] - own).astype(BF)
        more = dot(weight_s[slot][low:], kv)
        further = after[:, :1] + kept_s[slot][low:, :LANES].astype(F32)[:, :1]
        fresh = rows - low if first == "all" else ROWS if first else 0
        for at in range(low, rows, chunk):
            o, t = more[at - low : at - low + chunk], further[at - low : at - low + chunk]
            t = jnp.broadcast_to(t, (chunk, LANES))
            if at - low < fresh:
                acc_s[at : at + chunk] = o
                total_s[at : at + chunk] = t
            else:
                total = total_s[at : at + chunk]
                acc_s[at : at + chunk] = acc_s[at : at + chunk] + jnp.exp(-total) * o
                total_s[at : at + chunk] = total + t

    masks = [causal[at : at + chunk] for at in range(0, ROWS, chunk)]
    kv1, kv0 = keys_of(2 * z + 1), keys_of(2 * z)
    score_s[0][...] = scores(q_ref[...], kv1)
    score_s[1][...] = scores(q_ref[...], kv0)
    tile(0, kv1, ROWS, masks, "all")
    score_s[0][...] = scores(q_ref[...], keys_of(jnp.maximum(2 * z - 1, 0)))
    tile(1, kv0, 0, masks, True)

    def two(i, carry):
        j = 2 * (z - i) - 1
        score_s[1][...] = scores(q_ref[...], keys_of(j - 1))
        tile(0, keys_of(j), 0, [], False)
        score_s[0][...] = scores(q_ref[...], keys_of(jnp.maximum(j - 2, 0)))
        tile(1, keys_of(j - 1), 0, [], False)
        return carry

    lax.fori_loop(0, z, two, 0)
    low = lane_ids((ROWS // 2, LANES)) < HD
    for block in range(2):
        top = acc_s[block * ROWS : block * ROWS + ROWS // 2]
        bottom = acc_s[block * ROWS + ROWS // 2 : (block + 1) * ROWS]
        both = jnp.where(low, pltpu.roll(top, HD, 1), bottom).astype(BF)
        for peer in range(out_ref.shape[1]):
            out_ref[block, peer] = both


def route_body(col_ref, row_ref, col_out, row_out, *, experts, cap):
    below = (lane_ids((ROWS, ROWS)) < lax.broadcasted_iota(jnp.int32, (ROWS, ROWS), 0)).astype(F32).astype(BF)
    above = (lane_ids((ROWS, ROWS)) > lax.broadcasted_iota(jnp.int32, (ROWS, ROWS), 0)).astype(F32).astype(BF)
    ids = lane_ids((ROWS, LANES))
    hot = [(ids == col_ref[:, k : k + 1]).astype(F32) for k in range(2)]
    before = dot(below, (hot[0] + hot[1]).astype(BF))
    for k in range(2):
        place = jnp.sum(before * hot[k], axis=1, keepdims=True).astype(jnp.int32)
        col_out[:, k : k + 1] = col_ref[:, k : k + 1] * cap + place
    ids = lax.broadcasted_iota(jnp.int32, (experts, ROWS), 0)
    hot = [(ids == row_ref[k : k + 1]).astype(F32) for k in range(2)]
    before = dot((hot[0] + hot[1]).astype(BF), above)
    for k in range(2):
        place = jnp.sum(before * hot[k], axis=0, keepdims=True).astype(jnp.int32)
        row_out[k : k + 1] = row_ref[k : k + 1] * cap + place


def project_body(mixed_ref, ow_ref, res_ref, row_ref, stream_ref, out_ref):
    tp = ow_ref.shape[0]
    nothing = jnp.zeros((HD, LANES), BF)
    total = jnp.zeros((ROWS // 2, 2 * LANES), F32)
    for t in range(tp):
        pieces, weights = [], []
        for c in range(2):
            w = ow_ref[t, c * HD : (c + 1) * HD]
            pieces.append(mixed_ref[c * tp + t])
            weights.append(jnp.concatenate([w, nothing], axis=1))
            weights.append(jnp.concatenate([nothing, w], axis=1))
        total = total + dot(jnp.concatenate(pieces, axis=1), jnp.concatenate(weights, axis=0))
    attended = jnp.concatenate([total[:, :LANES], total[:, LANES:]], axis=0).astype(BF)
    stream = (res_ref[...].astype(F32) + attended.astype(F32)).astype(BF)
    stream_ref[...] = stream
    slots = lax.broadcasted_iota(jnp.int32, (out_ref.shape[0], ROWS), 0)
    owned = (slots == row_ref[0:1]) | (slots == row_ref[1:2])
    out_ref[...] = dot(owned.astype(F32).astype(BF), stream).astype(BF)


def plane(tp):
    side = int(tp**0.5)
    order = [list(range(tp)), [tp + v * side + u for u in range(side) for v in range(side)]]

    def pairs(shift):
        return [
            (group[u * side + v], group[u * side + (v + shift) % side])
            for group in order
            for u in range(side)
            for v in range(side)
        ]

    return side, order, pairs


def turned(t, side):
    return (t % side) * side + t // side


def weights_body(gate_ref, up_ref, down_ref, out_ref):
    for j in range(out_ref.shape[1]):
        at = slice(j * ROWS, (j + 1) * ROWS)
        out_ref[0, j] = gate_ref[at]
        out_ref[1, j] = up_ref[at]
        out_ref[2, j] = down_ref[:, at]


def expert_body(x_far, gain_ref, *rest):
    far, out_ref, near, x_ref, arrived = rest[:5], rest[5], rest[6:11], rest[11], rest[12]
    x_copy = pltpu.make_async_copy(x_far, x_ref, arrived.at[5])
    x_copy.start()
    copies = [pltpu.make_async_copy(f, n, arrived.at[i]) for i, (f, n) in enumerate(zip(far, near))]
    for c in copies:
        c.start()
    own_ref, left_ref, right_ref, front_ref, back_ref = near
    tp, rows = x_ref.shape[0] // 2, x_ref.shape[1]
    side = int(tp**0.5)
    x_copy.wait()
    wide = [jnp.concatenate([x_ref[i], x_ref[tp + turned(i, side)]], axis=0).astype(F32) for i in range(tp)]
    squares = wide[0] * wide[0]
    for w in wide[1:]:
        squares = squares + w * w
    mean = jnp.sum(squares, axis=1, keepdims=True) * (1.0 / (tp * LANES))
    factor = lax.rsqrt(mean + EPSILON)
    normed = [(w * factor * gain_ref[i : i + 1]).astype(BF) for i, w in enumerate(wide)]
    normed = jnp.concatenate(normed, axis=1)
    count = own_ref.shape[0] // 3

    def blocks(source, first, last):
        if source is not None:
            return source[first:last]
        half = front_ref.shape[0]
        if last <= half:
            return front_ref[first:last]
        if first >= half:
            return back_ref[first - half : last - half]
        return jnp.concatenate([front_ref[first:], back_ref[: last - half]], axis=0)

    sources = [own_ref, left_ref, right_ref, None]
    hidden = []
    for i, source in enumerate(sources):
        copies[i].wait()
        if source is None:
            copies[i + 1].wait()
        gate = dot(normed, blocks(source, 0, count).reshape(-1, ROWS))
        up = dot(normed, blocks(source, count, 2 * count).reshape(-1, ROWS))
        hidden.append((gate / (1.0 + jnp.exp(-gate)) * up).astype(BF))
    for j in range(count):
        total = dot(hidden[0], own_ref[2 * count + j])
        for h, source in zip(hidden[1:], sources[1:]):
            total = total + dot(h, blocks(source, 2 * count + j, 2 * count + j + 1)[0])
        for half in range(ROWS // LANES):
            t = j * (ROWS // LANES) + half
            share = total[:, half * LANES : (half + 1) * LANES].astype(BF)
            out_ref[t] = share[:rows]
            out_ref[tp + turned(t, side)] = share[rows:]


def spread_body(x_ref, out_ref):
    side = x_ref.shape[0]
    for c in range(2):
        for v in range(side):
            rows = jnp.concatenate([x_ref[v, z, c] for z in range(x_ref.shape[1])], axis=0)
            for u in range(side):
                out_ref[(c * side + u) * side + v] = rows


def sum_body(x_ref, out_ref):
    side, cap = out_ref.shape[0], out_ref.shape[3]
    for c in range(2):
        for v in range(side):
            pieces = [x_ref[(c * side + u) * side + v].astype(F32) for u in range(side)]
            total = pieces[0]
            for p in pieces[1:]:
                total = total + p
            total = total.astype(BF)
            for z in range(out_ref.shape[1]):
                out_ref[v, z, c] = total[z * cap : (z + 1) * cap]


def combine_body(x_ref, col_ref, score_ref, stream_ref, out_ref):
    x = x_ref[...]
    slots = lane_ids((ROWS, x.shape[0]))
    gap = score_ref[:, 0:1] - score_ref[:, 1:2]
    total = 0.0
    for k in range(2):
        owned = (slots == col_ref[:, k : k + 1]).astype(F32).astype(BF)
        share = 1.0 / (1.0 + jnp.exp(-gap if k == 0 else gap))
        total = total + share * dot(owned, x)
    out_ref[...] = (stream_ref[...].astype(F32) + total).astype(BF)


def shards(residual_in, queries, keys, values, out_weight, norm_gain, expert_routes, route_scores, gate_weight, up_weight, down_weight):
    zs, tp = lax.axis_size("z"), lax.axis_size("tp")
    experts = 2 * zs
    cap = 4 * ROWS // experts
    slots = experts * cap
    width = residual_in.shape[1]
    here = lax.axis_index("tp")

    packed = call(pack_body, shaped((2, 2, ROWS, LANES)), [VM] * 3)(queries, keys, values)
    packed = lax.all_to_all(packed, "core", 0, 0, tiled=True)
    side, order, pairs = plane(tp)
    both = ("core", "tp")
    blocks = width // ROWS
    step = blocks // 4
    own_kv = packed[:, 0].reshape(2 * ROWS, LANES)
    own_q = packed[:, 1].reshape(2 * ROWS, LANES)
    own_kv, gate_weight = lax.optimization_barrier((own_kv, gate_weight))
    own_w = pl.pallas_call(
        weights_body,
        out_shape=shaped((3, blocks, ROWS, ROWS)),
        grid=(4,),
        in_specs=[
            pl.BlockSpec((step * ROWS, ROWS), lambda i: (i, 0)),
            pl.BlockSpec((step * ROWS, ROWS), lambda i: (i, 0)),
            pl.BlockSpec((ROWS, step * ROWS), lambda i: (0, i)),
        ],
        out_specs=pl.BlockSpec((3, step, ROWS, ROWS), lambda i: (0, i, 0, 0)),
    )(gate_weight[0], up_weight[0], down_weight[0]).reshape(3 * blocks, ROWS, ROWS)
    left_w = lax.ppermute(own_w, both, pairs(1))
    right_w = lax.ppermute(own_w, both, pairs(-1))

    kv = lax.all_gather(own_kv, "z", axis=0, tiled=True)
    front_w = lax.ppermute(left_w[: 3 * blocks // 2], both, pairs(1))
    back_w = lax.ppermute(right_w[3 * blocks // 2 :], both, pairs(-1))
    kv, front_w, back_w = lax.optimization_barrier((kv, front_w, back_w))

    own_ow = jnp.moveaxis(out_weight.reshape(LANES, tp, LANES), 1, 0)
    own_ow = lax.all_to_all(own_ow, "tp", 0, 0, tiled=True)
    to_col, to_row = call(
        functools.partial(route_body, experts=experts, cap=cap),
        [shaped((ROWS, 2), jnp.int32), shaped((2, ROWS), jnp.int32)],
        [VM] * 2,
        out_specs=[VM] * 2,
    )(expert_routes, expert_routes.T)
    own_res = lax.dynamic_slice_in_dim(residual_in, here * LANES, LANES, 1)

    later = (lax.iota(jnp.int32, ROWS)[:, None] > lax.iota(jnp.int32, ROWS)[None, :]).astype(BF)
    place = lax.axis_index("z").reshape(1).astype(jnp.int32)
    mixed = call(
        attend_body,
        shaped((2, tp, ROWS // 2, LANES)),
        [SM] + [VM] * 3,
        scratch_shapes=[pltpu.VMEM((2 * ROWS, ROWS), F32)] * 4
        + [pltpu.VMEM((2 * ROWS, ROWS), BF)] * 4
        + [pltpu.VMEM((2 * ROWS, LANES), F32)] * 2,
    )(place, own_q, kv, later)
    mixed = lax.all_to_all(mixed.reshape(2 * tp, ROWS // 2, LANES), ("core", "tp"), 0, 0, tiled=True)

    stream, outgoing = call(
        project_body,
        [shaped((ROWS, LANES)), shaped((slots, LANES))],
        [VM] * 4,
        out_specs=[VM] * 2,
    )(mixed, own_ow, own_res, to_row)
    arrived = lax.all_to_all(outgoing.reshape(zs, 2, cap, LANES), "z", 0, 0, tiled=True)
    few = zs // side
    rows = few * cap
    copies = call(spread_body, shaped((2 * tp, rows, LANES)), [VM])(arrived.reshape(side, few, 2, cap, LANES))
    whole = [order[0] + order[1]]
    arrived = lax.all_to_all(copies, both, 0, 0, axis_index_groups=whole, tiled=True)
    weights = (own_w, left_w, right_w, front_w, back_w)
    parts = call(
        expert_body,
        shaped(arrived.shape),
        [pl.BlockSpec(memory_space=pl.ANY), VM] + [pl.BlockSpec(memory_space=pl.ANY)] * 5,
        scratch_shapes=[pltpu.VMEM(w.shape, BF) for w in weights]
        + [pltpu.VMEM(arrived.shape, BF), pltpu.SemaphoreType.DMA((6,))],
    )(arrived, norm_gain.reshape(tp, LANES), *weights)
    parts = lax.all_to_all(parts, both, 0, 0, axis_index_groups=whole, tiled=True)
    summed = call(sum_body, shaped((side, few, 2, cap, LANES)), [VM])(parts)
    returned = lax.all_to_all(summed.reshape(zs, 2, cap, LANES), "z", 0, 0, tiled=True)
    return call(combine_body, shaped((ROWS, LANES)), [VM] * 4)(
        returned.reshape(slots, LANES), to_col, route_scores, stream
    )


def solution(mesh):
    sp, tp = mesh.devices.shape
    fine = Mesh(mesh.devices.reshape(sp // 2, 2, tp), ("z", "core", "tp"))
    rows = ("z", "core")
    in_specs = (
        P(rows, None),
        P(rows, "tp"),
        P(rows, "tp"),
        P(rows, "tp"),
        P("tp", None),
        P(),
        P(rows, None),
        P(rows, None),
        P(rows, None, "tp"),
        P(rows, None, "tp"),
        P(rows, "tp", None),
    )
    return jax.shard_map(shards, mesh=fine, in_specs=in_specs, out_specs=P(rows, "tp"), check_vma=False)
```

```python
import functools

import jax
import jax.numpy as jnp
from jax import lax
from jax.experimental import pallas as pl
from jax.experimental.pallas import tpu as pltpu
from jax.sharding import Mesh, PartitionSpec as P

HD = 64
LANES = 128
ROWS = 256
EPSILON = 1e-06
BF = jnp.bfloat16
F32 = jnp.float32
VM = pl.BlockSpec(memory_space=pltpu.VMEM)
SM = pl.BlockSpec(memory_space=pltpu.SMEM)


def call(body, out_shape, specs, **more):
    return pl.pallas_call(body, out_shape=out_shape, in_specs=specs, **more)


def shaped(dims, dtype=BF):
    return jax.ShapeDtypeStruct(dims, dtype)


def lane_ids(dims):
    return lax.broadcasted_iota(jnp.int32, dims, len(dims) - 1)


def dot(a, b):
    return jnp.dot(a, b, preferred_element_type=F32)


def pack_body(q_ref, k_ref, v_ref, out_ref):
    q, k, v = (r[...].astype(F32) for r in (q_ref, k_ref, v_ref))
    low = lane_ids(q.shape) < HD
    q = q * (HD**-0.5)
    q_turned, k_turned, v_turned = (pltpu.roll(a, HD, 1) for a in (q, k, v))
    out_ref[0, 0] = jnp.where(low, k, v_turned).astype(BF)
    out_ref[1, 0] = jnp.where(low, k_turned, v).astype(BF)
    out_ref[0, 1] = jnp.where(low, q, 0.0).astype(BF)
    out_ref[1, 1] = jnp.where(low, q_turned, 0.0).astype(BF)


def scores(q, kv):
    return lax.dot_general(q, kv, (((1,), (1,)), ((), ())), preferred_element_type=F32)


def attend_body(z_ref, q_ref, kv_ref, later_ref, out_ref, *scratch):
    score_s, gap_s, kept_s, weight_s = (scratch[2 * i : 2 * i + 2] for i in range(4))
    acc_s, total_s = scratch[8:]
    z = z_ref[0]
    rows, chunk = 2 * ROWS, 64
    causal = lane_ids((ROWS, ROWS)) < lax.broadcasted_iota(jnp.int32, (ROWS, ROWS), 0)

    def keys_of(j):
        return kv_ref[pl.ds(pl.multiple_of(j * ROWS, ROWS), ROWS)]

    def tile(slot, kv, low, masks, first):
        for at in range(low, rows, chunk):
            s = score_s[slot][at : at + chunk]
            if at - low < len(masks) * chunk:
                s = jnp.where(masks[(at - low) // chunk], s, -1e30)
            kept = jnp.maximum(s, jnp.log(1.0 + jnp.exp(jnp.minimum(s, 80.0))))
            gap_s[slot][at : at + chunk] = s - kept
            kept_s[slot][at : at + chunk] = kept.astype(BF)
        after = dot(kept_s[slot][low:], later_ref[...])
        for at in range(low, rows, chunk):
            own = after[at - low : at - low + chunk]
            weight_s[slot][at : at + chunk] = jnp.exp(gap_s[slot][at : at + chunk] - own).astype(BF)
        more = dot(weight_s[slot][low:], kv)
        further = after[:, :1] + kept_s[slot][low:, :LANES].astype(F32)[:, :1]
        fresh = rows - low if first == "all" else ROWS if first else 0
        for at in range(low, rows, chunk):
            o, t = more[at - low : at - low + chunk], further[at - low : at - low + chunk]
            t = jnp.broadcast_to(t, (chunk, LANES))
            if at - low < fresh:
                acc_s[at : at + chunk] = o
                total_s[at : at + chunk] = t
            else:
                total = total_s[at : at + chunk]
                acc_s[at : at + chunk] = acc_s[at : at + chunk] + jnp.exp(-total) * o
                total_s[at : at + chunk] = total + t

    masks = [causal[at : at + chunk] for at in range(0, ROWS, chunk)]
    kv1, kv0 = keys_of(2 * z + 1), keys_of(2 * z)
    score_s[0][...] = scores(q_ref[...], kv1)
    score_s[1][...] = scores(q_ref[...], kv0)
    tile(0, kv1, ROWS, masks, "all")
    score_s[0][...] = scores(q_ref[...], keys_of(jnp.maximum(2 * z - 1, 0)))
    tile(1, kv0, 0, masks, True)

    def two(i, carry):
        j = 2 * (z - i) - 1
        score_s[1][...] = scores(q_ref[...], keys_of(j - 1))
        tile(0, keys_of(j), 0, [], False)
        score_s[0][...] = scores(q_ref[...], keys_of(jnp.maximum(j - 2, 0)))
        tile(1, keys_of(j - 1), 0, [], False)
        return carry

    lax.fori_loop(0, z, two, 0)
    low = lane_ids((ROWS // 2, LANES)) < HD
    for block in range(2):
        top = acc_s[block * ROWS : block * ROWS + ROWS // 2]
        bottom = acc_s[block * ROWS + ROWS // 2 : (block + 1) * ROWS]
        both = jnp.where(low, pltpu.roll(top, HD, 1), bottom).astype(BF)
        for peer in range(out_ref.shape[1]):
            out_ref[block, peer] = both


def route_body(col_ref, row_ref, col_out, row_out, *, experts, cap):
    below = (lane_ids((ROWS, ROWS)) < lax.broadcasted_iota(jnp.int32, (ROWS, ROWS), 0)).astype(F32).astype(BF)
    above = (lane_ids((ROWS, ROWS)) > lax.broadcasted_iota(jnp.int32, (ROWS, ROWS), 0)).astype(F32).astype(BF)
    ids = lane_ids((ROWS, LANES))
    hot = [(ids == col_ref[:, k : k + 1]).astype(F32) for k in range(2)]
    before = dot(below, (hot[0] + hot[1]).astype(BF))
    for k in range(2):
        place = jnp.sum(before * hot[k], axis=1, keepdims=True).astype(jnp.int32)
        col_out[:, k : k + 1] = col_ref[:, k : k + 1] * cap + place
    ids = lax.broadcasted_iota(jnp.int32, (experts, ROWS), 0)
    hot = [(ids == row_ref[k : k + 1]).astype(F32) for k in range(2)]
    before = dot((hot[0] + hot[1]).astype(BF), above)
    for k in range(2):
        place = jnp.sum(before * hot[k], axis=0, keepdims=True).astype(jnp.int32)
        row_out[k : k + 1] = row_ref[k : k + 1] * cap + place


def project_body(mixed_ref, ow_ref, res_ref, row_ref, stream_ref, out_ref):
    tp = ow_ref.shape[0]
    nothing = jnp.zeros((HD, LANES), BF)
    total = jnp.zeros((ROWS // 2, 2 * LANES), F32)
    for t in range(tp):
        pieces, weights = [], []
        for c in range(2):
            w = ow_ref[t, c * HD : (c + 1) * HD]
            pieces.append(mixed_ref[c * tp + t])
            weights.append(jnp.concatenate([w, nothing], axis=1))
            weights.append(jnp.concatenate([nothing, w], axis=1))
        total = total + dot(jnp.concatenate(pieces, axis=1), jnp.concatenate(weights, axis=0))
    attended = jnp.concatenate([total[:, :LANES], total[:, LANES:]], axis=0).astype(BF)
    stream = (res_ref[...].astype(F32) + attended.astype(F32)).astype(BF)
    stream_ref[...] = stream
    slots = lax.broadcasted_iota(jnp.int32, (out_ref.shape[0], ROWS), 0)
    owned = (slots == row_ref[0:1]) | (slots == row_ref[1:2])
    out_ref[...] = dot(owned.astype(F32).astype(BF), stream).astype(BF)


def plane(tp):
    side = int(tp**0.5)
    order = [list(range(tp)), [tp + v * side + u for u in range(side) for v in range(side)]]

    def pairs(shift):
        return [
            (group[u * side + v], group[u * side + (v + shift) % side])
            for group in order
            for u in range(side)
            for v in range(side)
        ]

    return side, order, pairs


def turned(t, side):
    return (t % side) * side + t // side


def weights_body(gate_ref, up_ref, down_ref, out_ref):
    for j in range(out_ref.shape[1]):
        at = slice(j * ROWS, (j + 1) * ROWS)
        out_ref[0, j] = gate_ref[at]
        out_ref[1, j] = up_ref[at]
        out_ref[2, j] = down_ref[:, at]


def expert_body(x_far, gain_ref, *rest):
    far, out_ref, near, x_ref, arrived = rest[:5], rest[5], rest[6:11], rest[11], rest[12]
    x_copy = pltpu.make_async_copy(x_far, x_ref, arrived.at[5])
    x_copy.start()
    copies = [pltpu.make_async_copy(f, n, arrived.at[i]) for i, (f, n) in enumerate(zip(far, near))]
    for c in copies:
        c.start()
    own_ref, left_ref, right_ref, front_ref, back_ref = near
    tp, rows = x_ref.shape[0] // 2, x_ref.shape[1]
    side = int(tp**0.5)
    x_copy.wait()
    wide = [jnp.concatenate([x_ref[i], x_ref[tp + turned(i, side)]], axis=0).astype(F32) for i in range(tp)]
    squares = wide[0] * wide[0]
    for w in wide[1:]:
        squares = squares + w * w
    mean = jnp.sum(squares, axis=1, keepdims=True) * (1.0 / (tp * LANES))
    factor = lax.rsqrt(mean + EPSILON)
    normed = [(w * factor * gain_ref[i : i + 1]).astype(BF) for i, w in enumerate(wide)]
    normed = jnp.concatenate(normed, axis=1)
    count = own_ref.shape[0] // 3

    def blocks(source, first, last):
        if source is not None:
            return source[first:last]
        half = front_ref.shape[0]
        if last <= half:
            return front_ref[first:last]
        if first >= half:
            return back_ref[first - half : last - half]
        return jnp.concatenate([front_ref[first:], back_ref[: last - half]], axis=0)

    sources = [own_ref, left_ref, right_ref, None]
    hidden = []
    for i, source in enumerate(sources):
        copies[i].wait()
        if source is None:
            copies[i + 1].wait()
        gate = dot(normed, blocks(source, 0, count).reshape(-1, ROWS))
        up = dot(normed, blocks(source, count, 2 * count).reshape(-1, ROWS))
        hidden.append((gate / (1.0 + jnp.exp(-gate)) * up).astype(BF))
    for j in range(count):
        total = dot(hidden[0], own_ref[2 * count + j])
        for h, source in zip(hidden[1:], sources[1:]):
            total = total + dot(h, blocks(source, 2 * count + j, 2 * count + j + 1)[0])
        for half in range(ROWS // LANES):
            t = j * (ROWS // LANES) + half
            share = total[:, half * LANES : (half + 1) * LANES].astype(BF)
            out_ref[t] = share[:rows]
            out_ref[tp + turned(t, side)] = share[rows:]


def spread_body(x_ref, out_ref):
    side = x_ref.shape[0]
    for c in range(2):
        for v in range(side):
            rows = jnp.concatenate([x_ref[v, z, c] for z in range(x_ref.shape[1])], axis=0)
            for u in range(side):
                out_ref[(c * side + u) * side + v] = rows


def sum_body(x_ref, out_ref):
    side, cap = out_ref.shape[0], out_ref.shape[3]
    for c in range(2):
        for v in range(side):
            pieces = [x_ref[(c * side + u) * side + v].astype(F32) for u in range(side)]
            total = pieces[0]
            for p in pieces[1:]:
                total = total + p
            total = total.astype(BF)
            for z in range(out_ref.shape[1]):
                out_ref[v, z, c] = total[z * cap : (z + 1) * cap]


def combine_body(x_ref, col_ref, score_ref, stream_ref, out_ref):
    x = x_ref[...]
    slots = lane_ids((ROWS, x.shape[0]))
    gap = score_ref[:, 0:1] - score_ref[:, 1:2]
    total = 0.0
    for k in range(2):
        owned = (slots == col_ref[:, k : k + 1]).astype(F32).astype(BF)
        share = 1.0 / (1.0 + jnp.exp(-gap if k == 0 else gap))
        total = total + share * dot(owned, x)
    out_ref[...] = (stream_ref[...].astype(F32) + total).astype(BF)


def shards(residual_in, queries, keys, values, out_weight, norm_gain, expert_routes, route_scores, gate_weight, up_weight, down_weight):
    zs, tp = lax.axis_size("z"), lax.axis_size("tp")
    experts = 2 * zs
    cap = 4 * ROWS // experts
    slots = experts * cap
    width = residual_in.shape[1]
    here = lax.axis_index("tp")

    packed = call(pack_body, shaped((2, 2, ROWS, LANES)), [VM] * 3)(queries, keys, values)
    packed = lax.all_to_all(packed, "core", 0, 0, tiled=True)
    side, order, pairs = plane(tp)
    both = ("core", "tp")
    blocks = width // ROWS
    step = blocks // 4
    own_kv = packed[:, 0].reshape(2 * ROWS, LANES)
    own_q = packed[:, 1].reshape(2 * ROWS, LANES)
    own_kv, gate_weight = lax.optimization_barrier((own_kv, gate_weight))
    own_w = pl.pallas_call(
        weights_body,
        out_shape=shaped((3, blocks, ROWS, ROWS)),
        grid=(4,),
        in_specs=[
            pl.BlockSpec((step * ROWS, ROWS), lambda i: (i, 0)),
            pl.BlockSpec((step * ROWS, ROWS), lambda i: (i, 0)),
            pl.BlockSpec((ROWS, step * ROWS), lambda i: (0, i)),
        ],
        out_specs=pl.BlockSpec((3, step, ROWS, ROWS), lambda i: (0, i, 0, 0)),
    )(gate_weight[0], up_weight[0], down_weight[0]).reshape(3 * blocks, ROWS, ROWS)
    left_w = lax.ppermute(own_w, both, pairs(1))
    right_w = lax.ppermute(own_w, both, pairs(-1))

    kv = lax.all_gather(own_kv, "z", axis=0, tiled=True)
    front_w = lax.ppermute(left_w[: 3 * blocks // 2], both, pairs(1))
    back_w = lax.ppermute(right_w[3 * blocks // 2 :], both, pairs(-1))

    own_ow = jnp.moveaxis(out_weight.reshape(LANES, tp, LANES), 1, 0)
    own_ow = lax.all_to_all(own_ow, "tp", 0, 0, tiled=True)
    to_col, to_row = call(
        functools.partial(route_body, experts=experts, cap=cap),
        [shaped((ROWS, 2), jnp.int32), shaped((2, ROWS), jnp.int32)],
        [VM] * 2,
        out_specs=[VM] * 2,
    )(expert_routes, expert_routes.T)
    own_res = lax.dynamic_slice_in_dim(residual_in, here * LANES, LANES, 1)

    later = (lax.iota(jnp.int32, ROWS)[:, None] > lax.iota(jnp.int32, ROWS)[None, :]).astype(BF)
    place = lax.axis_index("z").reshape(1).astype(jnp.int32)
    mixed = call(
        attend_body,
        shaped((2, tp, ROWS // 2, LANES)),
        [SM] + [VM] * 3,
        scratch_shapes=[pltpu.VMEM((2 * ROWS, ROWS), F32)] * 4
        + [pltpu.VMEM((2 * ROWS, ROWS), BF)] * 4
        + [pltpu.VMEM((2 * ROWS, LANES), F32)] * 2,
    )(place, own_q, kv, later)
    mixed, front_w, back_w = lax.optimization_barrier((mixed, front_w, back_w))
    mixed = lax.all_to_all(mixed.reshape(2 * tp, ROWS // 2, LANES), ("core", "tp"), 0, 0, tiled=True)

    stream, outgoing = call(
        project_body,
        [shaped((ROWS, LANES)), shaped((slots, LANES))],
        [VM] * 4,
        out_specs=[VM] * 2,
    )(mixed, own_ow, own_res, to_row)
    arrived = lax.all_to_all(outgoing.reshape(zs, 2, cap, LANES), "z", 0, 0, tiled=True)
    few = zs // side
    rows = few * cap
    copies = call(spread_body, shaped((2 * tp, rows, LANES)), [VM])(arrived.reshape(side, few, 2, cap, LANES))
    whole = [order[0] + order[1]]
    arrived = lax.all_to_all(copies, both, 0, 0, axis_index_groups=whole, tiled=True)
    weights = (own_w, left_w, right_w, front_w, back_w)
    parts = call(
        expert_body,
        shaped(arrived.shape),
        [pl.BlockSpec(memory_space=pl.ANY), VM] + [pl.BlockSpec(memory_space=pl.ANY)] * 5,
        scratch_shapes=[pltpu.VMEM(w.shape, BF) for w in weights]
        + [pltpu.VMEM(arrived.shape, BF), pltpu.SemaphoreType.DMA((6,))],
    )(arrived, norm_gain.reshape(tp, LANES), *weights)
    parts = lax.all_to_all(parts, both, 0, 0, axis_index_groups=whole, tiled=True)
    summed = call(sum_body, shaped((side, few, 2, cap, LANES)), [VM])(parts)
    returned = lax.all_to_all(summed.reshape(zs, 2, cap, LANES), "z", 0, 0, tiled=True)
    return call(combine_body, shaped((ROWS, LANES)), [VM] * 4)(
        returned.reshape(slots, LANES), to_col, route_scores, stream
    )


def solution(mesh):
    sp, tp = mesh.devices.shape
    fine = Mesh(mesh.devices.reshape(sp // 2, 2, tp), ("z", "core", "tp"))
    rows = ("z", "core")
    in_specs = (
        P(rows, None),
        P(rows, "tp"),
        P(rows, "tp"),
        P(rows, "tp"),
        P("tp", None),
        P(),
        P(rows, None),
        P(rows, None),
        P(rows, None, "tp"),
        P(rows, None, "tp"),
        P(rows, "tp", None),
    )
    return jax.shard_map(shards, mesh=fine, in_specs=in_specs, out_specs=P(rows, "tp"), check_vma=False)
```

```python
import functools

import jax
import jax.numpy as jnp
from jax import lax
from jax.experimental import pallas as pl
from jax.experimental.pallas import tpu as pltpu
from jax.sharding import Mesh, PartitionSpec as P

HD = 64
LANES = 128
ROWS = 256
EPSILON = 1e-06
BF = jnp.bfloat16
F32 = jnp.float32
VM = pl.BlockSpec(memory_space=pltpu.VMEM)
SM = pl.BlockSpec(memory_space=pltpu.SMEM)


def call(body, out_shape, specs, **more):
    return pl.pallas_call(body, out_shape=out_shape, in_specs=specs, **more)


def shaped(dims, dtype=BF):
    return jax.ShapeDtypeStruct(dims, dtype)


def lane_ids(dims):
    return lax.broadcasted_iota(jnp.int32, dims, len(dims) - 1)


def dot(a, b):
    return jnp.dot(a, b, preferred_element_type=F32)


def pack_body(q_ref, k_ref, v_ref, out_ref):
    q, k, v = (r[...].astype(F32) for r in (q_ref, k_ref, v_ref))
    low = lane_ids(q.shape) < HD
    q = q * (HD**-0.5)
    q_turned, k_turned, v_turned = (pltpu.roll(a, HD, 1) for a in (q, k, v))
    out_ref[0, 0] = jnp.where(low, k, v_turned).astype(BF)
    out_ref[1, 0] = jnp.where(low, k_turned, v).astype(BF)
    out_ref[0, 1] = jnp.where(low, q, 0.0).astype(BF)
    out_ref[1, 1] = jnp.where(low, q_turned, 0.0).astype(BF)


def scores(q, kv):
    return lax.dot_general(q, kv, (((1,), (1,)), ((), ())), preferred_element_type=F32)


def attend_body(z_ref, q_ref, kv_far, later_ref, out_ref, kv_ref, arrived, *scratch):
    score_s, gap_s, kept_s, weight_s = (scratch[2 * i : 2 * i + 2] for i in range(4))
    acc_s, total_s = scratch[8:]
    z = z_ref[0]
    rows, chunk = 2 * ROWS, 64
    causal = lane_ids((ROWS, ROWS)) < lax.broadcasted_iota(jnp.int32, (ROWS, ROWS), 0)

    def block_copy(b):
        at = pl.ds(pl.multiple_of(b * rows, rows), rows)
        return pltpu.make_async_copy(kv_far.at[at], kv_ref.at[at], arrived.at[b])

    def start(i, carry):
        block_copy(z - i).start()
        return carry

    lax.fori_loop(0, z + 1, start, 0)
    block_copy(z).wait()

    @pl.when(z > 0)
    def _():
        block_copy(z - 1).wait()

    def keys_of(j):
        return kv_ref[pl.ds(pl.multiple_of(j * ROWS, ROWS), ROWS)]

    def tile(slot, kv, low, masks, first):
        for at in range(low, rows, chunk):
            s = score_s[slot][at : at + chunk]
            if at - low < len(masks) * chunk:
                s = jnp.where(masks[(at - low) // chunk], s, -1e30)
            kept = jnp.maximum(s, jnp.log(1.0 + jnp.exp(jnp.minimum(s, 80.0))))
            gap_s[slot][at : at + chunk] = s - kept
            kept_s[slot][at : at + chunk] = kept.astype(BF)
        after = dot(kept_s[slot][low:], later_ref[...])
        for at in range(low, rows, chunk):
            own = after[at - low : at - low + chunk]
            weight_s[slot][at : at + chunk] = jnp.exp(gap_s[slot][at : at + chunk] - own).astype(BF)
        more = dot(weight_s[slot][low:], kv)
        further = after[:, :1] + kept_s[slot][low:, :LANES].astype(F32)[:, :1]
        fresh = rows - low if first == "all" else ROWS if first else 0
        for at in range(low, rows, chunk):
            o, t = more[at - low : at - low + chunk], further[at - low : at - low + chunk]
            t = jnp.broadcast_to(t, (chunk, LANES))
            if at - low < fresh:
                acc_s[at : at + chunk] = o
                total_s[at : at + chunk] = t
            else:
                total = total_s[at : at + chunk]
                acc_s[at : at + chunk] = acc_s[at : at + chunk] + jnp.exp(-total) * o
                total_s[at : at + chunk] = total + t

    masks = [causal[at : at + chunk] for at in range(0, ROWS, chunk)]
    kv1, kv0 = keys_of(2 * z + 1), keys_of(2 * z)
    score_s[0][...] = scores(q_ref[...], kv1)
    score_s[1][...] = scores(q_ref[...], kv0)
    tile(0, kv1, ROWS, masks, "all")
    score_s[0][...] = scores(q_ref[...], keys_of(jnp.maximum(2 * z - 1, 0)))
    tile(1, kv0, 0, masks, True)

    def two(i, carry):
        j = 2 * (z - i) - 1

        @pl.when(i + 1 < z)
        def _():
            block_copy(z - i - 2).wait()

        score_s[1][...] = scores(q_ref[...], keys_of(j - 1))
        tile(0, keys_of(j), 0, [], False)
        score_s[0][...] = scores(q_ref[...], keys_of(jnp.maximum(j - 2, 0)))
        tile(1, keys_of(j - 1), 0, [], False)
        return carry

    lax.fori_loop(0, z, two, 0)
    low = lane_ids((ROWS // 2, LANES)) < HD
    for block in range(2):
        top = acc_s[block * ROWS : block * ROWS + ROWS // 2]
        bottom = acc_s[block * ROWS + ROWS // 2 : (block + 1) * ROWS]
        both = jnp.where(low, pltpu.roll(top, HD, 1), bottom).astype(BF)
        for peer in range(out_ref.shape[1]):
            out_ref[block, peer] = both


def route_body(col_ref, row_ref, col_out, row_out, *, experts, cap):
    below = (lane_ids((ROWS, ROWS)) < lax.broadcasted_iota(jnp.int32, (ROWS, ROWS), 0)).astype(F32).astype(BF)
    above = (lane_ids((ROWS, ROWS)) > lax.broadcasted_iota(jnp.int32, (ROWS, ROWS), 0)).astype(F32).astype(BF)
    ids = lane_ids((ROWS, LANES))
    hot = [(ids == col_ref[:, k : k + 1]).astype(F32) for k in range(2)]
    before = dot(below, (hot[0] + hot[1]).astype(BF))
    for k in range(2):
        place = jnp.sum(before * hot[k], axis=1, keepdims=True).astype(jnp.int32)
        col_out[:, k : k + 1] = col_ref[:, k : k + 1] * cap + place
    ids = lax.broadcasted_iota(jnp.int32, (experts, ROWS), 0)
    hot = [(ids == row_ref[k : k + 1]).astype(F32) for k in range(2)]
    before = dot((hot[0] + hot[1]).astype(BF), above)
    for k in range(2):
        place = jnp.sum(before * hot[k], axis=0, keepdims=True).astype(jnp.int32)
        row_out[k : k + 1] = row_ref[k : k + 1] * cap + place


def project_body(mixed_far, ow_ref, res_ref, row_ref, stream_ref, out_ref, mixed_ref, arrived):
    tp = ow_ref.shape[0]
    copies = []
    for i in range(4):
        for c in range(2):
            at = pl.ds(c * tp + i * (tp // 4), tp // 4)
            copies.append(pltpu.make_async_copy(mixed_far.at[at], mixed_ref.at[at], arrived.at[2 * i + c]))
    for c in copies:
        c.start()
    nothing = jnp.zeros((HD, LANES), BF)
    total = jnp.zeros((ROWS // 2, 2 * LANES), F32)
    for t in range(tp):
        if t % (tp // 4) == 0:
            for c in range(2):
                copies[t // (tp // 4) * 2 + c].wait()
        pieces, weights = [], []
        for c in range(2):
            w = ow_ref[t, c * HD : (c + 1) * HD]
            pieces.append(mixed_ref[c * tp + t])
            weights.append(jnp.concatenate([w, nothing], axis=1))
            weights.append(jnp.concatenate([nothing, w], axis=1))
        total = total + dot(jnp.concatenate(pieces, axis=1), jnp.concatenate(weights, axis=0))
    attended = jnp.concatenate([total[:, :LANES], total[:, LANES:]], axis=0).astype(BF)
    stream = (res_ref[...].astype(F32) + attended.astype(F32)).astype(BF)
    stream_ref[...] = stream
    slots = lax.broadcasted_iota(jnp.int32, (out_ref.shape[0], ROWS), 0)
    owned = (slots == row_ref[0:1]) | (slots == row_ref[1:2])
    out_ref[...] = dot(owned.astype(F32).astype(BF), stream).astype(BF)


def plane(tp):
    side = int(tp**0.5)
    order = [list(range(tp)), [tp + v * side + u for u in range(side) for v in range(side)]]

    def pairs(shift):
        return [
            (group[u * side + v], group[u * side + (v + shift) % side])
            for group in order
            for u in range(side)
            for v in range(side)
        ]

    return side, order, pairs


def turned(t, side):
    return (t % side) * side + t // side


def weights_body(gate_ref, up_ref, down_ref, out_ref):
    for j in range(out_ref.shape[1]):
        at = slice(j * ROWS, (j + 1) * ROWS)
        out_ref[0, j] = gate_ref[at]
        out_ref[1, j] = up_ref[at]
        out_ref[2, j] = down_ref[:, at]


def expert_body(core_ref, x_far, gain_ref, *rest, cap):
    far, out_ref, near, x_ref, arrived = rest[:5], rest[5], rest[6:11], rest[11], rest[12]
    x_copy = pltpu.make_async_copy(x_far, x_ref, arrived.at[5])
    x_copy.start()
    copies = [pltpu.make_async_copy(f, n, arrived.at[i]) for i, (f, n) in enumerate(zip(far, near))]
    for c in copies:
        c.start()
    own_ref, left_ref, right_ref, front_ref, back_ref = near
    tp = x_ref.shape[0]
    side, core = int(tp**0.5), core_ref[0]
    x_copy.wait()
    wide = [x_ref[jnp.where(core == 1, turned(i, side), i)].astype(F32) for i in range(tp)]
    squares = wide[0] * wide[0]
    for w in wide[1:]:
        squares = squares + w * w
    mean = jnp.sum(squares, axis=1, keepdims=True) * (1.0 / (tp * LANES))
    factor = lax.rsqrt(mean + EPSILON)
    normed = [(w * factor * gain_ref[i : i + 1]).astype(BF) for i, w in enumerate(wide)]
    normed = jnp.concatenate(normed, axis=1)
    count = own_ref.shape[0] // 3

    def blocks(source, first, last):
        if source is not None:
            return source[first:last]
        half = front_ref.shape[0]
        if last <= half:
            return front_ref[first:last]
        if first >= half:
            return back_ref[first - half : last - half]
        return jnp.concatenate([front_ref[first:], back_ref[: last - half]], axis=0)

    sources = [own_ref, left_ref, right_ref, None]
    hidden = []
    for i, source in enumerate(sources):
        copies[i].wait()
        if source is None:
            copies[i + 1].wait()
        gate = dot(normed, blocks(source, 0, count).reshape(-1, ROWS))
        up = dot(normed, blocks(source, count, 2 * count).reshape(-1, ROWS))
        hidden.append((gate / (1.0 + jnp.exp(-gate)) * up).astype(BF))
    for j in range(count):
        total = dot(hidden[0], own_ref[2 * count + j])
        for h, source in zip(hidden[1:], sources[1:]):
            total = total + dot(h, blocks(source, 2 * count + j, 2 * count + j + 1)[0])
        for half in range(ROWS // LANES):
            t = j * (ROWS // LANES) + half
            share = total[:, half * LANES : (half + 1) * LANES].astype(BF)
            for z in range(out_ref.shape[1] // cap):
                at = 2 * cap * z
                out_ref[t, z * cap : (z + 1) * cap] = share[at : at + cap]
                out_ref[tp + turned(t, side), z * cap : (z + 1) * cap] = share[at + cap : at + 2 * cap]


def sum_body(x_ref, out_ref):
    side, cap = out_ref.shape[0], out_ref.shape[3]
    for c in range(2):
        for v in range(side):
            pieces = [x_ref[(c * side + u) * side + v].astype(F32) for u in range(side)]
            total = pieces[0]
            for p in pieces[1:]:
                total = total + p
            total = total.astype(BF)
            for z in range(out_ref.shape[1]):
                out_ref[v, z, c] = total[z * cap : (z + 1) * cap]


def combine_body(x_ref, col_ref, score_ref, stream_ref, out_ref):
    x = x_ref[...]
    slots = lane_ids((ROWS, x.shape[0]))
    gap = score_ref[:, 0:1] - score_ref[:, 1:2]
    total = 0.0
    for k in range(2):
        owned = (slots == col_ref[:, k : k + 1]).astype(F32).astype(BF)
        share = 1.0 / (1.0 + jnp.exp(-gap if k == 0 else gap))
        total = total + share * dot(owned, x)
    out_ref[...] = (stream_ref[...].astype(F32) + total).astype(BF)


def shards(residual_in, queries, keys, values, out_weight, norm_gain, expert_routes, route_scores, gate_weight, up_weight, down_weight):
    zs, tp = lax.axis_size("z"), lax.axis_size("tp")
    experts = 2 * zs
    cap = 4 * ROWS // experts
    slots = experts * cap
    width = residual_in.shape[1]
    here = lax.axis_index("tp")

    packed = call(pack_body, shaped((2, 2, ROWS, LANES)), [VM] * 3)(queries, keys, values)
    packed = lax.all_to_all(packed, "core", 0, 0, tiled=True)
    side, order, pairs = plane(tp)
    both = ("core", "tp")
    blocks = width // ROWS
    step = blocks // 4
    own_kv = packed[:, 0].reshape(2 * ROWS, LANES)
    own_q = packed[:, 1].reshape(2 * ROWS, LANES)
    own_kv, gate_weight = lax.optimization_barrier((own_kv, gate_weight))
    own_w = pl.pallas_call(
        weights_body,
        out_shape=shaped((3, blocks, ROWS, ROWS)),
        grid=(4,),
        in_specs=[
            pl.BlockSpec((step * ROWS, ROWS), lambda i: (i, 0)),
            pl.BlockSpec((step * ROWS, ROWS), lambda i: (i, 0)),
            pl.BlockSpec((ROWS, step * ROWS), lambda i: (0, i)),
        ],
        out_specs=pl.BlockSpec((3, step, ROWS, ROWS), lambda i: (0, i, 0, 0)),
    )(gate_weight[0], up_weight[0], down_weight[0]).reshape(3 * blocks, ROWS, ROWS)
    left_w = lax.ppermute(own_w, both, pairs(1))
    right_w = lax.ppermute(own_w, both, pairs(-1))

    kv = lax.all_gather(own_kv, "z", axis=0, tiled=True)
    front_w = lax.ppermute(left_w[: 3 * blocks // 2], both, pairs(1))
    back_w = lax.ppermute(right_w[3 * blocks // 2 :], both, pairs(-1))

    own_ow = jnp.moveaxis(out_weight.reshape(LANES, tp, LANES), 1, 0)
    own_ow = lax.all_to_all(own_ow, "tp", 0, 0, tiled=True)
    to_col, to_row = call(
        functools.partial(route_body, experts=experts, cap=cap),
        [shaped((ROWS, 2), jnp.int32), shaped((2, ROWS), jnp.int32)],
        [VM] * 2,
        out_specs=[VM] * 2,
    )(expert_routes, expert_routes.T)
    own_res = lax.dynamic_slice_in_dim(residual_in, here * LANES, LANES, 1)

    later = (lax.iota(jnp.int32, ROWS)[:, None] > lax.iota(jnp.int32, ROWS)[None, :]).astype(BF)
    place = lax.axis_index("z").reshape(1).astype(jnp.int32)
    mixed = call(
        attend_body,
        shaped((2, tp, ROWS // 2, LANES)),
        [SM, VM, pl.BlockSpec(memory_space=pl.ANY), VM],
        scratch_shapes=[pltpu.VMEM(kv.shape, BF), pltpu.SemaphoreType.DMA((zs,))]
        + [pltpu.VMEM((2 * ROWS, ROWS), F32)] * 4
        + [pltpu.VMEM((2 * ROWS, ROWS), BF)] * 4
        + [pltpu.VMEM((2 * ROWS, LANES), F32)] * 2,
    )(place, own_q, kv, later)
    mixed, front_w, back_w = lax.optimization_barrier((mixed, front_w, back_w))
    mixed = lax.all_to_all(mixed.reshape(2 * tp, ROWS // 2, LANES), ("core", "tp"), 0, 0, tiled=True)

    stream, outgoing = call(
        project_body,
        [shaped((ROWS, LANES)), shaped((slots, LANES))],
        [pl.BlockSpec(memory_space=pl.ANY)] + [VM] * 3,
        out_specs=[VM] * 2,
        scratch_shapes=[pltpu.VMEM(mixed.shape, BF), pltpu.SemaphoreType.DMA((8,))],
    )(mixed, own_ow, own_res, to_row)
    arrived = lax.all_to_all(outgoing.reshape(experts, cap, LANES), ("z", "core"), 0, 0, tiled=True)
    few = zs // side
    rows = 2 * few * cap
    copies = jnp.broadcast_to(arrived.reshape(1, side, rows, LANES), (side, side, rows, LANES))
    arrived = lax.all_to_all(copies.reshape(tp, rows, LANES), both, 0, 0, axis_index_groups=order, tiled=True)
    core = lax.axis_index("core").reshape(1).astype(jnp.int32)
    weights = (own_w, left_w, right_w, front_w, back_w)
    parts = call(
        functools.partial(expert_body, cap=cap),
        shaped((2 * tp, few * cap, LANES)),
        [SM, pl.BlockSpec(memory_space=pl.ANY), VM] + [pl.BlockSpec(memory_space=pl.ANY)] * 5,
        scratch_shapes=[pltpu.VMEM(w.shape, BF) for w in weights]
        + [pltpu.VMEM(arrived.shape, BF), pltpu.SemaphoreType.DMA((6,))],
    )(core, arrived, norm_gain.reshape(tp, LANES), *weights)
    whole = [order[0] + order[1]]
    parts = lax.all_to_all(parts, both, 0, 0, axis_index_groups=whole, tiled=True)
    summed = call(sum_body, shaped((side, few, 2, cap, LANES)), [VM])(parts)
    returned = lax.all_to_all(summed.reshape(zs, 2, cap, LANES), "z", 0, 0, tiled=True)
    return call(combine_body, shaped((ROWS, LANES)), [VM] * 4)(
        returned.reshape(slots, LANES), to_col, route_scores, stream
    )


def solution(mesh):
    sp, tp = mesh.devices.shape
    fine = Mesh(mesh.devices.reshape(sp // 2, 2, tp), ("z", "core", "tp"))
    rows = ("z", "core")
    in_specs = (
        P(rows, None),
        P(rows, "tp"),
        P(rows, "tp"),
        P(rows, "tp"),
        P("tp", None),
        P(),
        P(rows, None),
        P(rows, None),
        P(rows, None, "tp"),
        P(rows, None, "tp"),
        P(rows, "tp", None),
    )
    return jax.shard_map(shards, mesh=fine, in_specs=in_specs, out_specs=P(rows, "tp"), check_vma=False)
```

```python
import functools

import jax
import jax.numpy as jnp
from jax import lax
from jax.experimental import pallas as pl
from jax.experimental.pallas import tpu as pltpu
from jax.sharding import Mesh, PartitionSpec as P

HD = 64
LANES = 128
ROWS = 256
EPSILON = 1e-06
BF = jnp.bfloat16
F32 = jnp.float32
VM = pl.BlockSpec(memory_space=pltpu.VMEM)
SM = pl.BlockSpec(memory_space=pltpu.SMEM)


def call(body, out_shape, specs, limit=24, **more):
    params = pltpu.CompilerParams(vmem_limit_bytes=limit << 20) if limit else None
    return pl.pallas_call(body, out_shape=out_shape, in_specs=specs, compiler_params=params, **more)


def shaped(dims, dtype=BF):
    return jax.ShapeDtypeStruct(dims, dtype)


def lane_ids(dims):
    return lax.broadcasted_iota(jnp.int32, dims, len(dims) - 1)


def dot(a, b):
    return jnp.dot(a, b, preferred_element_type=F32)


def pack_body(q_ref, k_ref, v_ref, out_ref):
    q, k, v = (r[...].astype(F32) for r in (q_ref, k_ref, v_ref))
    low = lane_ids(q.shape) < HD
    q = q * (HD**-0.5)
    q_turned, k_turned, v_turned = (pltpu.roll(a, HD, 1) for a in (q, k, v))
    out_ref[0, 0] = jnp.where(low, k, v_turned).astype(BF)
    out_ref[1, 0] = jnp.where(low, k_turned, v).astype(BF)
    out_ref[0, 1] = jnp.where(low, q, 0.0).astype(BF)
    out_ref[1, 1] = jnp.where(low, q_turned, 0.0).astype(BF)


def scores(q, kv):
    return lax.dot_general(q, kv, (((1,), (1,)), ((), ())), preferred_element_type=F32)


def attend_body(z_ref, q_ref, kv_ref, later_ref, out_ref, *scratch):
    score_s, gap_s, kept_s, weight_s = (scratch[2 * i : 2 * i + 2] for i in range(4))
    acc_s, total_s = scratch[8:]
    z = z_ref[0]
    rows, chunk = 2 * ROWS, 64
    causal = lane_ids((ROWS, ROWS)) < lax.broadcasted_iota(jnp.int32, (ROWS, ROWS), 0)

    def keys_of(j):
        return kv_ref[pl.ds(pl.multiple_of(j * ROWS, ROWS), ROWS)]

    def tile(slot, kv, low, masks, first):
        for at in range(low, rows, chunk):
            s = score_s[slot][at : at + chunk]
            if at - low < len(masks) * chunk:
                s = jnp.where(masks[(at - low) // chunk], s, -1e30)
            kept = jnp.maximum(s, jnp.log(1.0 + jnp.exp(jnp.minimum(s, 80.0))))
            gap_s[slot][at : at + chunk] = s - kept
            kept_s[slot][at : at + chunk] = kept.astype(BF)
        after = dot(kept_s[slot][low:], later_ref[...])
        for at in range(low, rows, chunk):
            own = after[at - low : at - low + chunk]
            weight_s[slot][at : at + chunk] = jnp.exp(gap_s[slot][at : at + chunk] - own).astype(BF)
        more = dot(weight_s[slot][low:], kv)
        further = after[:, :1] + kept_s[slot][low:, :LANES].astype(F32)[:, :1]
        fresh = rows - low if first == "all" else ROWS if first else 0
        for at in range(low, rows, chunk):
            o, t = more[at - low : at - low + chunk], further[at - low : at - low + chunk]
            t = jnp.broadcast_to(t, (chunk, LANES))
            if at - low < fresh:
                acc_s[at : at + chunk] = o
                total_s[at : at + chunk] = t
            else:
                total = total_s[at : at + chunk]
                acc_s[at : at + chunk] = acc_s[at : at + chunk] + jnp.exp(-total) * o
                total_s[at : at + chunk] = total + t

    masks = [causal[at : at + chunk] for at in range(0, ROWS, chunk)]
    kv1, kv0 = keys_of(2 * z + 1), keys_of(2 * z)
    score_s[0][...] = scores(q_ref[...], kv1)
    score_s[1][...] = scores(q_ref[...], kv0)
    tile(0, kv1, ROWS, masks, "all")
    score_s[0][...] = scores(q_ref[...], keys_of(jnp.maximum(2 * z - 1, 0)))
    tile(1, kv0, 0, masks, True)

    def two(i, carry):
        j = 2 * (z - i) - 1
        score_s[1][...] = scores(q_ref[...], keys_of(j - 1))
        tile(0, keys_of(j), 0, [], False)
        score_s[0][...] = scores(q_ref[...], keys_of(jnp.maximum(j - 2, 0)))
        tile(1, keys_of(j - 1), 0, [], False)
        return carry

    lax.fori_loop(0, z, two, 0)
    low = lane_ids((ROWS // 2, LANES)) < HD
    for block in range(2):
        top = acc_s[block * ROWS : block * ROWS + ROWS // 2]
        bottom = acc_s[block * ROWS + ROWS // 2 : (block + 1) * ROWS]
        both = jnp.where(low, pltpu.roll(top, HD, 1), bottom).astype(BF)
        for peer in range(out_ref.shape[1]):
            out_ref[block, peer] = both


def route_body(col_ref, row_ref, col_out, row_out, *, experts, cap):
    below = (lane_ids((ROWS, ROWS)) < lax.broadcasted_iota(jnp.int32, (ROWS, ROWS), 0)).astype(F32).astype(BF)
    above = (lane_ids((ROWS, ROWS)) > lax.broadcasted_iota(jnp.int32, (ROWS, ROWS), 0)).astype(F32).astype(BF)
    ids = lane_ids((ROWS, LANES))
    hot = [(ids == col_ref[:, k : k + 1]).astype(F32) for k in range(2)]
    before = dot(below, (hot[0] + hot[1]).astype(BF))
    for k in range(2):
        place = jnp.sum(before * hot[k], axis=1, keepdims=True).astype(jnp.int32)
        col_out[:, k : k + 1] = col_ref[:, k : k + 1] * cap + place
    ids = lax.broadcasted_iota(jnp.int32, (experts, ROWS), 0)
    hot = [(ids == row_ref[k : k + 1]).astype(F32) for k in range(2)]
    before = dot((hot[0] + hot[1]).astype(BF), above)
    for k in range(2):
        place = jnp.sum(before * hot[k], axis=0, keepdims=True).astype(jnp.int32)
        row_out[k : k + 1] = row_ref[k : k + 1] * cap + place


def project_body(mixed_ref, ow_ref, res_ref, row_ref, stream_ref, out_ref):
    tp = ow_ref.shape[0]
    nothing = jnp.zeros((HD, LANES), BF)
    total = jnp.zeros((ROWS // 2, 2 * LANES), F32)
    for t in range(tp):
        pieces, weights = [], []
        for c in range(2):
            w = ow_ref[t, c * HD : (c + 1) * HD]
            pieces.append(mixed_ref[c * tp + t])
            weights.append(jnp.concatenate([w, nothing], axis=1))
            weights.append(jnp.concatenate([nothing, w], axis=1))
        total = total + dot(jnp.concatenate(pieces, axis=1), jnp.concatenate(weights, axis=0))
    attended = jnp.concatenate([total[:, :LANES], total[:, LANES:]], axis=0).astype(BF)
    stream = (res_ref[...].astype(F32) + attended.astype(F32)).astype(BF)
    stream_ref[...] = stream
    slots = lax.broadcasted_iota(jnp.int32, (out_ref.shape[0], ROWS), 0)
    owned = (slots == row_ref[0:1]) | (slots == row_ref[1:2])
    out_ref[...] = dot(owned.astype(F32).astype(BF), stream).astype(BF)


def plane(tp):
    side = int(tp**0.5)
    order = [list(range(tp)), [tp + v * side + u for u in range(side) for v in range(side)]]

    def pairs(shift):
        return [
            (group[u * side + v], group[u * side + (v + shift) % side])
            for group in order
            for u in range(side)
            for v in range(side)
        ]

    return side, order, pairs


def turned(t, side):
    return (t % side) * side + t // side


def weights_body(gate_ref, up_ref, down_ref, out_ref):
    for j in range(out_ref.shape[1]):
        at = slice(j * ROWS, (j + 1) * ROWS)
        out_ref[0, j] = gate_ref[at]
        out_ref[1, j] = up_ref[at]
        out_ref[2, j] = down_ref[:, at]


def expert_body(x_far, gain_ref, *rest):
    far, out_ref, near, x_ref, arrived = rest[:5], rest[5], rest[6:11], rest[11], rest[12]
    x_copy = pltpu.make_async_copy(x_far, x_ref, arrived.at[5])
    x_copy.start()
    copies = [pltpu.make_async_copy(f, n, arrived.at[i]) for i, (f, n) in enumerate(zip(far, near))]
    for c in copies:
        c.start()
    own_ref, left_ref, right_ref, front_ref, back_ref = near
    tp, rows = x_ref.shape[0] // 2, x_ref.shape[1]
    side = int(tp**0.5)
    x_copy.wait()
    wide = [jnp.concatenate([x_ref[i], x_ref[tp + turned(i, side)]], axis=0).astype(F32) for i in range(tp)]
    squares = wide[0] * wide[0]
    for w in wide[1:]:
        squares = squares + w * w
    mean = jnp.sum(squares, axis=1, keepdims=True) * (1.0 / (tp * LANES))
    factor = lax.rsqrt(mean + EPSILON)
    normed = [(w * factor * gain_ref[i : i + 1]).astype(BF) for i, w in enumerate(wide)]
    normed = jnp.concatenate(normed, axis=1)
    count = own_ref.shape[0] // 3

    def blocks(source, first, last):
        if source is not None:
            return source[first:last]
        half = front_ref.shape[0]
        if last <= half:
            return front_ref[first:last]
        if first >= half:
            return back_ref[first - half : last - half]
        return jnp.concatenate([front_ref[first:], back_ref[: last - half]], axis=0)

    sources = [own_ref, left_ref, right_ref, None]
    hidden = []
    for i, source in enumerate(sources):
        copies[i].wait()
        if source is None:
            copies[i + 1].wait()
        gate = dot(normed, blocks(source, 0, count).reshape(-1, ROWS))
        up = dot(normed, blocks(source, count, 2 * count).reshape(-1, ROWS))
        hidden.append((gate / (1.0 + jnp.exp(-gate)) * up).astype(BF))
    for j in range(count):
        total = dot(hidden[0], own_ref[2 * count + j])
        for h, source in zip(hidden[1:], sources[1:]):
            total = total + dot(h, blocks(source, 2 * count + j, 2 * count + j + 1)[0])
        for half in range(ROWS // LANES):
            t = j * (ROWS // LANES) + half
            share = total[:, half * LANES : (half + 1) * LANES].astype(BF)
            out_ref[t] = share[:rows]
            out_ref[tp + turned(t, side)] = share[rows:]


def spread_body(x_ref, out_ref):
    side = x_ref.shape[0]
    for c in range(2):
        for v in range(side):
            rows = jnp.concatenate([x_ref[v, z, c] for z in range(x_ref.shape[1])], axis=0)
            for u in range(side):
                out_ref[(c * side + u) * side + v] = rows


def sum_body(x_ref, out_ref):
    side, cap = out_ref.shape[0], out_ref.shape[3]
    for c in range(2):
        for v in range(side):
            pieces = [x_ref[(c * side + u) * side + v].astype(F32) for u in range(side)]
            total = pieces[0]
            for p in pieces[1:]:
                total = total + p
            total = total.astype(BF)
            for z in range(out_ref.shape[1]):
                out_ref[v, z, c] = total[z * cap : (z + 1) * cap]


def combine_body(x_ref, col_ref, score_ref, stream_ref, out_ref):
    x = x_ref[...]
    slots = lane_ids((ROWS, x.shape[0]))
    gap = score_ref[:, 0:1] - score_ref[:, 1:2]
    total = 0.0
    for k in range(2):
        owned = (slots == col_ref[:, k : k + 1]).astype(F32).astype(BF)
        share = 1.0 / (1.0 + jnp.exp(-gap if k == 0 else gap))
        total = total + share * dot(owned, x)
    out_ref[...] = (stream_ref[...].astype(F32) + total).astype(BF)


def shards(residual_in, queries, keys, values, out_weight, norm_gain, expert_routes, route_scores, gate_weight, up_weight, down_weight):
    zs, tp = lax.axis_size("z"), lax.axis_size("tp")
    experts = 2 * zs
    cap = 4 * ROWS // experts
    slots = experts * cap
    width = residual_in.shape[1]
    here = lax.axis_index("tp")

    packed = call(pack_body, shaped((2, 2, ROWS, LANES)), [VM] * 3)(queries, keys, values)
    packed = lax.all_to_all(packed, "core", 0, 0, tiled=True)
    side, order, pairs = plane(tp)
    both = ("core", "tp")
    blocks = width // ROWS
    step = blocks // 4
    own_kv = packed[:, 0].reshape(2 * ROWS, LANES)
    own_q = packed[:, 1].reshape(2 * ROWS, LANES)
    own_kv, gate_weight = lax.optimization_barrier((own_kv, gate_weight))
    own_w = pl.pallas_call(
        weights_body,
        out_shape=shaped((3, blocks, ROWS, ROWS)),
        grid=(4,),
        in_specs=[
            pl.BlockSpec((step * ROWS, ROWS), lambda i: (i, 0)),
            pl.BlockSpec((step * ROWS, ROWS), lambda i: (i, 0)),
            pl.BlockSpec((ROWS, step * ROWS), lambda i: (0, i)),
        ],
        out_specs=pl.BlockSpec((3, step, ROWS, ROWS), lambda i: (0, i, 0, 0)),
    )(gate_weight[0], up_weight[0], down_weight[0]).reshape(3 * blocks, ROWS, ROWS)
    left_w = lax.ppermute(own_w, both, pairs(1))
    right_w = lax.ppermute(own_w, both, pairs(-1))

    kv = lax.all_gather(own_kv, "z", axis=0, tiled=True)
    front_w = lax.ppermute(left_w[: 3 * blocks // 2], both, pairs(1))
    back_w = lax.ppermute(right_w[3 * blocks // 2 :], both, pairs(-1))

    own_ow = jnp.moveaxis(out_weight.reshape(LANES, tp, LANES), 1, 0)
    own_ow = lax.all_to_all(own_ow, "tp", 0, 0, tiled=True)
    to_col, to_row = call(
        functools.partial(route_body, experts=experts, cap=cap),
        [shaped((ROWS, 2), jnp.int32), shaped((2, ROWS), jnp.int32)],
        [VM] * 2,
        out_specs=[VM] * 2,
    )(expert_routes, expert_routes.T)
    own_res = lax.dynamic_slice_in_dim(residual_in, here * LANES, LANES, 1)

    later = (lax.iota(jnp.int32, ROWS)[:, None] > lax.iota(jnp.int32, ROWS)[None, :]).astype(BF)
    place = lax.axis_index("z").reshape(1).astype(jnp.int32)
    mixed = call(
        attend_body,
        shaped((2, tp, ROWS // 2, LANES)),
        [SM] + [VM] * 3,
        limit=None,
        scratch_shapes=[pltpu.VMEM((2 * ROWS, ROWS), F32)] * 4
        + [pltpu.VMEM((2 * ROWS, ROWS), BF)] * 4
        + [pltpu.VMEM((2 * ROWS, LANES), F32)] * 2,
    )(place, own_q, kv, later)
    mixed, front_w, back_w = lax.optimization_barrier((mixed, front_w, back_w))
    mixed = lax.all_to_all(mixed.reshape(2 * tp, ROWS // 2, LANES), ("core", "tp"), 0, 0, tiled=True)

    stream, outgoing = call(
        project_body,
        [shaped((ROWS, LANES)), shaped((slots, LANES))],
        [VM] * 4,
        out_specs=[VM] * 2,
    )(mixed, own_ow, own_res, to_row)
    arrived = lax.all_to_all(outgoing.reshape(zs, 2, cap, LANES), "z", 0, 0, tiled=True)
    few = zs // side
    rows = few * cap
    copies = call(spread_body, shaped((2 * tp, rows, LANES)), [VM])(arrived.reshape(side, few, 2, cap, LANES))
    whole = [order[0] + order[1]]
    arrived = lax.all_to_all(copies, both, 0, 0, axis_index_groups=whole, tiled=True)
    weights = (own_w, left_w, right_w, front_w, back_w)
    parts = call(
        expert_body,
        shaped(arrived.shape),
        [pl.BlockSpec(memory_space=pl.ANY), VM] + [pl.BlockSpec(memory_space=pl.ANY)] * 5,
        limit=None,
        scratch_shapes=[pltpu.VMEM(w.shape, BF) for w in weights]
        + [pltpu.VMEM(arrived.shape, BF), pltpu.SemaphoreType.DMA((6,))],
    )(arrived, norm_gain.reshape(tp, LANES), *weights)
    parts = lax.all_to_all(parts, both, 0, 0, axis_index_groups=whole, tiled=True)
    summed = call(sum_body, shaped((side, few, 2, cap, LANES)), [VM])(parts)
    returned = lax.all_to_all(summed.reshape(zs, 2, cap, LANES), "z", 0, 0, tiled=True)
    return call(combine_body, shaped((ROWS, LANES)), [VM] * 4)(
        returned.reshape(slots, LANES), to_col, route_scores, stream
    )


def solution(mesh):
    sp, tp = mesh.devices.shape
    fine = Mesh(mesh.devices.reshape(sp // 2, 2, tp), ("z", "core", "tp"))
    rows = ("z", "core")
    in_specs = (
        P(rows, None),
        P(rows, "tp"),
        P(rows, "tp"),
        P(rows, "tp"),
        P("tp", None),
        P(),
        P(rows, None),
        P(rows, None),
        P(rows, None, "tp"),
        P(rows, None, "tp"),
        P(rows, "tp", None),
    )
    return jax.shard_map(shards, mesh=fine, in_specs=in_specs, out_specs=P(rows, "tp"), check_vma=False)
```

```python
import functools

import jax
import jax.numpy as jnp
from jax import lax
from jax.experimental import pallas as pl
from jax.experimental.pallas import tpu as pltpu
from jax.sharding import Mesh, PartitionSpec as P

HD = 64
LANES = 128
ROWS = 256
EPSILON = 1e-06
BF = jnp.bfloat16
F32 = jnp.float32
VM = pl.BlockSpec(memory_space=pltpu.VMEM)
SM = pl.BlockSpec(memory_space=pltpu.SMEM)


def call(body, out_shape, specs, limit=24, **more):
    params = pltpu.CompilerParams(vmem_limit_bytes=limit << 20) if limit else None
    return pl.pallas_call(body, out_shape=out_shape, in_specs=specs, compiler_params=params, **more)


def shaped(dims, dtype=BF):
    return jax.ShapeDtypeStruct(dims, dtype)


def lane_ids(dims):
    return lax.broadcasted_iota(jnp.int32, dims, len(dims) - 1)


def dot(a, b):
    return jnp.dot(a, b, preferred_element_type=F32)


def pack_body(q_ref, k_ref, v_ref, out_ref):
    q, k, v = (r[...].astype(F32) for r in (q_ref, k_ref, v_ref))
    low = lane_ids(q.shape) < HD
    q = q * (HD**-0.5)
    q_turned, k_turned, v_turned = (pltpu.roll(a, HD, 1) for a in (q, k, v))
    out_ref[0, 0] = jnp.where(low, k, v_turned).astype(BF)
    out_ref[1, 0] = jnp.where(low, k_turned, v).astype(BF)
    out_ref[0, 1] = jnp.where(low, q, 0.0).astype(BF)
    out_ref[1, 1] = jnp.where(low, q_turned, 0.0).astype(BF)


def scores(q, kv):
    return lax.dot_general(q, kv, (((1,), (1,)), ((), ())), preferred_element_type=F32)


def attend_body(z_ref, q_ref, kv_ref, later_ref, out_ref, *scratch):
    score_s, gap_s, kept_s, weight_s = (scratch[2 * i : 2 * i + 2] for i in range(4))
    acc_s, total_s = scratch[8:]
    z = z_ref[0]
    rows, chunk = 2 * ROWS, 64
    causal = lane_ids((ROWS, ROWS)) < lax.broadcasted_iota(jnp.int32, (ROWS, ROWS), 0)

    def keys_of(j):
        return kv_ref[pl.ds(pl.multiple_of(j * ROWS, ROWS), ROWS)]

    def tile(slot, kv, low, masks, first):
        for at in range(low, rows, chunk):
            s = score_s[slot][at : at + chunk]
            if at - low < len(masks) * chunk:
                s = jnp.where(masks[(at - low) // chunk], s, -1e30)
            kept = jnp.maximum(s, jnp.log(1.0 + jnp.exp(jnp.minimum(s, 80.0))))
            gap_s[slot][at : at + chunk] = s - kept
            kept_s[slot][at : at + chunk] = kept.astype(BF)
        after = dot(kept_s[slot][low:], later_ref[...])
        for at in range(low, rows, chunk):
            own = after[at - low : at - low + chunk]
            weight_s[slot][at : at + chunk] = jnp.exp(gap_s[slot][at : at + chunk] - own).astype(BF)
        more = dot(weight_s[slot][low:], kv)
        further = after[:, :1] + kept_s[slot][low:, :LANES].astype(F32)[:, :1]
        fresh = rows - low if first == "all" else ROWS if first else 0
        for at in range(low, rows, chunk):
            o, t = more[at - low : at - low + chunk], further[at - low : at - low + chunk]
            t = jnp.broadcast_to(t, (chunk, LANES))
            if at - low < fresh:
                acc_s[at : at + chunk] = o
                total_s[at : at + chunk] = t
            else:
                total = total_s[at : at + chunk]
                acc_s[at : at + chunk] = acc_s[at : at + chunk] + jnp.exp(-total) * o
                total_s[at : at + chunk] = total + t

    masks = [causal[at : at + chunk] for at in range(0, ROWS, chunk)]
    kv1, kv0 = keys_of(2 * z + 1), keys_of(2 * z)
    score_s[0][...] = scores(q_ref[...], kv1)
    score_s[1][...] = scores(q_ref[...], kv0)
    tile(0, kv1, ROWS, masks, "all")
    score_s[0][...] = scores(q_ref[...], keys_of(jnp.maximum(2 * z - 1, 0)))
    tile(1, kv0, 0, masks, True)

    def two(i, carry):
        j = 2 * (z - i) - 1
        score_s[1][...] = scores(q_ref[...], keys_of(j - 1))
        tile(0, keys_of(j), 0, [], False)
        score_s[0][...] = scores(q_ref[...], keys_of(jnp.maximum(j - 2, 0)))
        tile(1, keys_of(j - 1), 0, [], False)
        return carry

    lax.fori_loop(0, z, two, 0)
    low = lane_ids((ROWS // 2, LANES)) < HD
    for block in range(2):
        top = acc_s[block * ROWS : block * ROWS + ROWS // 2]
        bottom = acc_s[block * ROWS + ROWS // 2 : (block + 1) * ROWS]
        both = jnp.where(low, pltpu.roll(top, HD, 1), bottom).astype(BF)
        for peer in range(out_ref.shape[1]):
            out_ref[block, peer] = both


def route_body(col_ref, row_ref, col_out, row_out, *, experts, cap):
    below = (lane_ids((ROWS, ROWS)) < lax.broadcasted_iota(jnp.int32, (ROWS, ROWS), 0)).astype(F32).astype(BF)
    above = (lane_ids((ROWS, ROWS)) > lax.broadcasted_iota(jnp.int32, (ROWS, ROWS), 0)).astype(F32).astype(BF)
    ids = lane_ids((ROWS, LANES))
    hot = [(ids == col_ref[:, k : k + 1]).astype(F32) for k in range(2)]
    before = dot(below, (hot[0] + hot[1]).astype(BF))
    for k in range(2):
        place = jnp.sum(before * hot[k], axis=1, keepdims=True).astype(jnp.int32)
        col_out[:, k : k + 1] = col_ref[:, k : k + 1] * cap + place
    ids = lax.broadcasted_iota(jnp.int32, (experts, ROWS), 0)
    hot = [(ids == row_ref[k : k + 1]).astype(F32) for k in range(2)]
    before = dot((hot[0] + hot[1]).astype(BF), above)
    for k in range(2):
        place = jnp.sum(before * hot[k], axis=0, keepdims=True).astype(jnp.int32)
        row_out[k : k + 1] = row_ref[k : k + 1] * cap + place


def project_body(mixed_ref, ow_ref, res_ref, row_ref, stream_ref, out_ref):
    tp = ow_ref.shape[0]
    nothing = jnp.zeros((HD, LANES), BF)
    total = jnp.zeros((ROWS // 2, 2 * LANES), F32)
    for t in range(tp):
        pieces, weights = [], []
        for c in range(2):
            w = ow_ref[t, c * HD : (c + 1) * HD]
            pieces.append(mixed_ref[c * tp + t])
            weights.append(jnp.concatenate([w, nothing], axis=1))
            weights.append(jnp.concatenate([nothing, w], axis=1))
        total = total + dot(jnp.concatenate(pieces, axis=1), jnp.concatenate(weights, axis=0))
    attended = jnp.concatenate([total[:, :LANES], total[:, LANES:]], axis=0).astype(BF)
    stream = (res_ref[...].astype(F32) + attended.astype(F32)).astype(BF)
    stream_ref[...] = stream
    slots = lax.broadcasted_iota(jnp.int32, (out_ref.shape[0], ROWS), 0)
    owned = (slots == row_ref[0:1]) | (slots == row_ref[1:2])
    out_ref[...] = dot(owned.astype(F32).astype(BF), stream).astype(BF)


def plane(tp):
    side = int(tp**0.5)
    order = [list(range(tp)), [tp + v * side + u for u in range(side) for v in range(side)]]

    def pairs(shift):
        return [
            (group[u * side + v], group[u * side + (v + shift) % side])
            for group in order
            for u in range(side)
            for v in range(side)
        ]

    return side, order, pairs


def turned(t, side):
    return (t % side) * side + t // side


def weights_body(gate_ref, up_ref, down_ref, out_ref):
    for j in range(out_ref.shape[1]):
        at = slice(j * ROWS, (j + 1) * ROWS)
        out_ref[0, j] = gate_ref[at]
        out_ref[1, j] = up_ref[at]
        out_ref[2, j] = down_ref[:, at]


def expert_body(x_ref, gain_ref, *rest):
    far, out_ref, near, arrived = rest[:5], rest[5], rest[6:11], rest[11]
    copies = [pltpu.make_async_copy(f, n, arrived.at[i]) for i, (f, n) in enumerate(zip(far, near))]
    for c in copies:
        c.start()
    own_ref, left_ref, right_ref, front_ref, back_ref = near
    tp, rows = x_ref.shape[0] // 2, x_ref.shape[1]
    side = int(tp**0.5)
    wide = [jnp.concatenate([x_ref[i], x_ref[tp + turned(i, side)]], axis=0).astype(F32) for i in range(tp)]
    squares = wide[0] * wide[0]
    for w in wide[1:]:
        squares = squares + w * w
    mean = jnp.sum(squares, axis=1, keepdims=True) * (1.0 / (tp * LANES))
    factor = lax.rsqrt(mean + EPSILON)
    normed = [(w * factor * gain_ref[i : i + 1]).astype(BF) for i, w in enumerate(wide)]
    normed = jnp.concatenate(normed, axis=1)
    count = own_ref.shape[0] // 3

    def blocks(source, first, last):
        if source is not None:
            return source[first:last]
        half = front_ref.shape[0]
        if last <= half:
            return front_ref[first:last]
        if first >= half:
            return back_ref[first - half : last - half]
        return jnp.concatenate([front_ref[first:], back_ref[: last - half]], axis=0)

    sources = [own_ref, left_ref, right_ref, None]
    hidden = []
    for i, source in enumerate(sources):
        copies[i].wait()
        if source is None:
            copies[i + 1].wait()
        gate = dot(normed, blocks(source, 0, count).reshape(-1, ROWS))
        up = dot(normed, blocks(source, count, 2 * count).reshape(-1, ROWS))
        hidden.append((gate / (1.0 + jnp.exp(-gate)) * up).astype(BF))
    for j in range(count):
        total = dot(hidden[0], own_ref[2 * count + j])
        for h, source in zip(hidden[1:], sources[1:]):
            total = total + dot(h, blocks(source, 2 * count + j, 2 * count + j + 1)[0])
        for half in range(ROWS // LANES):
            t = j * (ROWS // LANES) + half
            share = total[:, half * LANES : (half + 1) * LANES].astype(BF)
            out_ref[t] = share[:rows]
            out_ref[tp + turned(t, side)] = share[rows:]


def spread_body(x_ref, out_ref):
    side = x_ref.shape[0]
    for c in range(2):
        for v in range(side):
            rows = jnp.concatenate([x_ref[v, z, c] for z in range(x_ref.shape[1])], axis=0)
            for u in range(side):
                out_ref[(c * side + u) * side + v] = rows


def sum_body(x_ref, out_ref):
    side, cap = out_ref.shape[0], out_ref.shape[3]
    for c in range(2):
        for v in range(side):
            pieces = [x_ref[(c * side + u) * side + v].astype(F32) for u in range(side)]
            total = pieces[0]
            for p in pieces[1:]:
                total = total + p
            total = total.astype(BF)
            for z in range(out_ref.shape[1]):
                out_ref[v, z, c] = total[z * cap : (z + 1) * cap]


def combine_body(x_ref, col_ref, score_ref, stream_ref, out_ref):
    x = x_ref[...]
    slots = lane_ids((ROWS, x.shape[0]))
    gap = score_ref[:, 0:1] - score_ref[:, 1:2]
    total = 0.0
    for k in range(2):
        owned = (slots == col_ref[:, k : k + 1]).astype(F32).astype(BF)
        share = 1.0 / (1.0 + jnp.exp(-gap if k == 0 else gap))
        total = total + share * dot(owned, x)
    out_ref[...] = (stream_ref[...].astype(F32) + total).astype(BF)


def shards(residual_in, queries, keys, values, out_weight, norm_gain, expert_routes, route_scores, gate_weight, up_weight, down_weight):
    zs, tp = lax.axis_size("z"), lax.axis_size("tp")
    experts = 2 * zs
    cap = 4 * ROWS // experts
    slots = experts * cap
    width = residual_in.shape[1]
    here = lax.axis_index("tp")

    packed = call(pack_body, shaped((2, 2, ROWS, LANES)), [VM] * 3)(queries, keys, values)
    packed = lax.all_to_all(packed, "core", 0, 0, tiled=True)
    side, order, pairs = plane(tp)
    both = ("core", "tp")
    blocks = width // ROWS
    step = blocks // 4
    own_kv = packed[:, 0].reshape(2 * ROWS, LANES)
    own_q = packed[:, 1].reshape(2 * ROWS, LANES)
    own_kv, gate_weight = lax.optimization_barrier((own_kv, gate_weight))
    own_w = pl.pallas_call(
        weights_body,
        out_shape=shaped((3, blocks, ROWS, ROWS)),
        grid=(4,),
        in_specs=[
            pl.BlockSpec((step * ROWS, ROWS), lambda i: (i, 0)),
            pl.BlockSpec((step * ROWS, ROWS), lambda i: (i, 0)),
            pl.BlockSpec((ROWS, step * ROWS), lambda i: (0, i)),
        ],
        out_specs=pl.BlockSpec((3, step, ROWS, ROWS), lambda i: (0, i, 0, 0)),
    )(gate_weight[0], up_weight[0], down_weight[0]).reshape(3 * blocks, ROWS, ROWS)
    left_w = lax.ppermute(own_w, both, pairs(1))
    right_w = lax.ppermute(own_w, both, pairs(-1))

    kv = lax.all_gather(own_kv, "z", axis=0, tiled=True)
    front_w = lax.ppermute(left_w[: 3 * blocks // 2], both, pairs(1))
    back_w = lax.ppermute(right_w[3 * blocks // 2 :], both, pairs(-1))

    own_ow = jnp.moveaxis(out_weight.reshape(LANES, tp, LANES), 1, 0)
    own_ow = lax.all_to_all(own_ow, "tp", 0, 0, tiled=True)
    to_col, to_row = call(
        functools.partial(route_body, experts=experts, cap=cap),
        [shaped((ROWS, 2), jnp.int32), shaped((2, ROWS), jnp.int32)],
        [VM] * 2,
        out_specs=[VM] * 2,
    )(expert_routes, expert_routes.T)
    own_res = lax.dynamic_slice_in_dim(residual_in, here * LANES, LANES, 1)

    later = (lax.iota(jnp.int32, ROWS)[:, None] > lax.iota(jnp.int32, ROWS)[None, :]).astype(BF)
    place = lax.axis_index("z").reshape(1).astype(jnp.int32)
    mixed = call(
        attend_body,
        shaped((2, tp, ROWS // 2, LANES)),
        [SM] + [VM] * 3,
        limit=None,
        scratch_shapes=[pltpu.VMEM((2 * ROWS, ROWS), F32)] * 4
        + [pltpu.VMEM((2 * ROWS, ROWS), BF)] * 4
        + [pltpu.VMEM((2 * ROWS, LANES), F32)] * 2,
    )(place, own_q, kv, later)
    mixed, front_w, back_w = lax.optimization_barrier((mixed, front_w, back_w))
    mixed = lax.all_to_all(mixed.reshape(2 * tp, ROWS // 2, LANES), ("core", "tp"), 0, 0, tiled=True)

    stream, outgoing = call(
        project_body,
        [shaped((ROWS, LANES)), shaped((slots, LANES))],
        [VM] * 4,
        out_specs=[VM] * 2,
    )(mixed, own_ow, own_res, to_row)
    arrived = lax.all_to_all(outgoing.reshape(zs, 2, cap, LANES), "z", 0, 0, tiled=True)
    few = zs // side
    rows = few * cap
    copies = call(spread_body, shaped((2 * tp, rows, LANES)), [VM])(arrived.reshape(side, few, 2, cap, LANES))
    whole = [order[0] + order[1]]
    arrived = lax.all_to_all(copies, both, 0, 0, axis_index_groups=whole, tiled=True)
    weights = (own_w, left_w, right_w, front_w, back_w)
    parts = call(
        expert_body,
        shaped(arrived.shape),
        [VM] * 2 + [pl.BlockSpec(memory_space=pl.ANY)] * 5,
        limit=44,
        scratch_shapes=[pltpu.VMEM(w.shape, BF) for w in weights] + [pltpu.SemaphoreType.DMA((5,))],
    )(arrived, norm_gain.reshape(tp, LANES), *weights)
    parts = lax.all_to_all(parts, both, 0, 0, axis_index_groups=whole, tiled=True)
    summed = call(sum_body, shaped((side, few, 2, cap, LANES)), [VM])(parts)
    returned = lax.all_to_all(summed.reshape(zs, 2, cap, LANES), "z", 0, 0, tiled=True)
    return call(combine_body, shaped((ROWS, LANES)), [VM] * 4)(
        returned.reshape(slots, LANES), to_col, route_scores, stream
    )


def solution(mesh):
    sp, tp = mesh.devices.shape
    fine = Mesh(mesh.devices.reshape(sp // 2, 2, tp), ("z", "core", "tp"))
    rows = ("z", "core")
    in_specs = (
        P(rows, None),
        P(rows, "tp"),
        P(rows, "tp"),
        P(rows, "tp"),
        P("tp", None),
        P(),
        P(rows, None),
        P(rows, None),
        P(rows, None, "tp"),
        P(rows, None, "tp"),
        P(rows, "tp", None),
    )
    return jax.shard_map(shards, mesh=fine, in_specs=in_specs, out_specs=P(rows, "tp"), check_vma=False)
```
